32 devices in a mesh: rep: 2 (over x), fs: 8 (over z, y), tp: 2 (over core).
Axes of the slice: x: 2, y: 2, z: 4, core: 2. Of those that a mesh axis runs over, the one named last changes fastest.
Arguments:
- inputs: bfloat16 [8192, 2048], P(('rep', 'fs')), may hold values from -6 to 6
- cotangent: bfloat16 [8192, 2048], P(('rep', 'fs')), may hold values from -6 to 6
- gate_pre: bfloat16 [8192, 5632], P(('rep', 'fs'), 'tp'), may hold values from -8 to 8
- up_pre: bfloat16 [8192, 5632], P(('rep', 'fs'), 'tp'), may hold values from -6 to 6
- gate_weight: float32 [2048, 5632], P('fs', 'tp'), may hold values from -0.125 to 0.125
- up_weight: float32 [2048, 5632], P('fs', 'tp'), may hold values from -0.125 to 0.125
- down_weight: float32 [2048, 5632], P('fs', 'tp'), may hold values from -0.078125 to 0.078125
- gate_scale: float32 [1, 5632], P(None, 'tp'), may hold values from 0.1 to 1.9
- up_scale: float32 [1, 5632], P(None, 'tp'), may hold values from 0.1 to 1.9
- down_scale: float32 [1, 5632], P(None, 'tp'), may hold values from 0.1 to 1.9
Outputs:
- input_grad: bfloat16 [8192, 2048], P(('rep', 'fs'), 'tp')
- gate_grad: float32 [2048, 5632], P('fs', 'tp')
- up_grad: float32 [2048, 5632], P('fs', 'tp')
- down_grad: float32 [2048, 5632], P('fs', 'tp')
The draws below stay inside these ranges and needn't reach their ends.
All inputs are finite; a program needn't handle non-finite values.
Results may differ from the reference program's by a relative error of at most 0.018.
Values may be sent and summed in bfloat16 or wider, within the bound.
A program may use at most 192 MiB of HBM per device.

```python
import jax
import jax.numpy as jnp
from jax import lax

D = 2048
FF = 5632
TOKENS = 8192
N_TP = 2


def spiked(array, own_key, source, target, blocks, factor):
    owner, partner = [(jnp.arange(array.shape[position]) // (array.shape[position] // blocks)).reshape([-1 if axis == position else 1 for axis in range(array.ndim)]) for position in (source, target)]
    chosen = jax.random.permutation(own_key, blocks)[partner]
    strong = (owner == chosen) | (owner == (partner + blocks // 2) % blocks)
    return jnp.where(strong, factor * array, array)


def level_of(key, extent, shards, least, top_value):
    factor_of, own = 1.0, jax.random.fold_in(key, 6)
    for axis_at, parts in shards:
        draws = jnp.exp(jax.random.uniform(jax.random.fold_in(own, axis_at), (parts,), jnp.float32, least / len(shards), top_value / len(shards)))
        factor_of = factor_of * jnp.repeat(draws, extent[axis_at] // parts).reshape([-1 if axis == axis_at else 1 for axis in range(len(extent))])
    return factor_of


def normal_values(own_key, extent, scale, reach, shards=(), kind=jnp.bfloat16):
    level = level_of(own_key, extent, shards, -0.22, 0.18) if shards else 1.0
    entries = jax.random.normal(own_key, extent, jnp.float32) * scale * level
    return jnp.minimum(jnp.maximum(entries, -reach), reach).astype(kind)


def heavy_noise(own_key, extent, deviation, reach, pieces, heavy, kind=jnp.bfloat16):
    result = deviation * jax.random.normal(own_key, extent, jnp.float32)
    if pieces:
        result = result * level_of(own_key, extent, pieces, -0.22, 0.18)
    return jnp.clip(spiked(result, jax.random.fold_in(own_key, 3), *heavy), -reach, reach).astype(kind)


def setup_inputs(seed: int = 0) -> dict:
    arg_keys = jax.random.split(jax.random.key(seed), 11)
    inputs = normal_values(arg_keys[0], (TOKENS, D), 1.0, 6.0, ((0, 16),))
    cotangent = heavy_noise(arg_keys[1], (TOKENS, D), 1.0, 6.0, ((0, 16),), (0, 1, 16, 2.0))
    gate_pre = normal_values(arg_keys[2], (TOKENS, FF), 1.5, 8.0, ((0, 16), (1, 2)))
    up_pre = normal_values(arg_keys[3], (TOKENS, FF), 1.0, 6.0, ((0, 16), (1, 2)))
    gate_weight = normal_values(arg_keys[4], (D, FF), D ** -0.5, 0.125, ((0, 8), (1, 2)), jnp.float32)
    up_weight = normal_values(arg_keys[5], (D, FF), D ** -0.5, 0.125, ((0, 8), (1, 2)), jnp.float32)
    down_weight = normal_values(arg_keys[6], (D, FF), FF ** -0.5, 0.078125, ((0, 8), (1, 2)), jnp.float32)
    gate_scale = jnp.clip(1.0 + 0.18 * jax.random.normal(arg_keys[7], (1, FF), jnp.float32), 0.1, 1.9)
    up_scale = jnp.clip(1.0 + 0.18 * jax.random.normal(arg_keys[8], (1, FF), jnp.float32), 0.1, 1.9)
    down_scale = jnp.clip(1.0 + 0.18 * jax.random.normal(arg_keys[9], (1, FF), jnp.float32), 0.1, 1.9)
    return dict(inputs=inputs, cotangent=cotangent, gate_pre=gate_pre, up_pre=up_pre, gate_weight=gate_weight, up_weight=up_weight, down_weight=down_weight, gate_scale=gate_scale, up_scale=up_scale, down_scale=down_scale)


def reference(inputs, cotangent, gate_pre, up_pre, gate_weight, up_weight, down_weight, gate_scale, up_scale, down_scale):
    gate = gate_pre.astype(jnp.float32)
    upper = up_pre.astype(jnp.float32)
    sig = jax.nn.sigmoid(gate)
    act = gate * sig
    hidden = (act * upper).astype(jnp.bfloat16)
    down_bf = down_weight.astype(jnp.bfloat16)
    hidden_cot = jnp.dot(cotangent, down_bf, preferred_element_type=jnp.float32) * down_scale
    gate_cot = (hidden_cot * upper * sig * (1.0 + gate * (1.0 - sig)) * gate_scale).astype(jnp.bfloat16)
    up_cot = (hidden_cot * act * up_scale).astype(jnp.bfloat16)
    width = FF // N_TP
    gate_bf = gate_weight.astype(jnp.bfloat16)
    up_bf = up_weight.astype(jnp.bfloat16)

    def block_sum(total, index):
        start = (index * width).astype(jnp.int32)
        gc = lax.dynamic_slice_in_dim(gate_cot, start, width, 1)
        uc = lax.dynamic_slice_in_dim(up_cot, start, width, 1)
        gw = lax.dynamic_slice_in_dim(gate_bf, start, width, 1)
        uw = lax.dynamic_slice_in_dim(up_bf, start, width, 1)
        part = jnp.dot(gc, gw.T, preferred_element_type=jnp.float32) + jnp.dot(uc, uw.T, preferred_element_type=jnp.float32)
        return total + part.astype(jnp.bfloat16).astype(jnp.float32), None

    summed, _ = lax.scan(block_sum, jnp.zeros((TOKENS, D), jnp.float32), jnp.arange(N_TP, dtype=jnp.int32))
    input_grad = summed.astype(jnp.bfloat16)
    gate_grad = jnp.dot(inputs.T, gate_cot, preferred_element_type=jnp.float32)
    up_grad = jnp.dot(inputs.T, up_cot, preferred_element_type=jnp.float32)
    down_grad = jnp.dot(cotangent.T, hidden, preferred_element_type=jnp.float32) * down_scale
    return (input_grad, gate_grad, up_grad, down_grad)
```

```python
import functools

import jax
import jax.numpy as jnp
from jax import lax
from jax.experimental import pallas as pl
from jax.experimental.pallas import tpu as pltpu
from jax.sharding import PartitionSpec as P


BF = jnp.bfloat16
F32 = jnp.float32


def local(
    n_rep,
    n_fs,
    n_tp,
    inputs,
    cotangent,
    gate_pre,
    up_pre,
    gate_weight,
    up_weight,
    down_weight,
    gate_scale,
    up_scale,
    down_scale,
):
    n_out = 4 if n_fs % 4 == 0 else 1
    n_in = n_fs // n_out
    tokens = inputs.shape[0]
    width = inputs.shape[1]
    block = width // n_fs
    part = gate_pre.shape[1] // n_rep
    r = lax.axis_index("rep")
    f = lax.axis_index("fs")
    t = lax.axis_index("tp")
    zo, yo = f // n_in, f % n_in

    def from_rep(value, k):
        return lax.ppermute(value, "rep", [((i + k) % n_rep, i) for i in range(n_rep)])

    def from_tp(value, k):
        return lax.ppermute(value, "tp", [((i + k) % n_tp, i) for i in range(n_tp)])

    def from_outer(value, k):
        pairs = [
            (((z + k) % n_out) * n_in + y, z * n_in + y)
            for z in range(n_out)
            for y in range(n_in)
        ]
        return lax.ppermute(value, "fs", pairs)

    def from_inner(value, k):
        pairs = [
            (z * n_in + (y + k) % n_in, z * n_in + y)
            for z in range(n_out)
            for y in range(n_in)
        ]
        return lax.ppermute(value, "fs", pairs)

    def column_part(value, index):
        return lax.dynamic_slice_in_dim(value, index * part, part, 1)

    def spread_tokens(value):
        return jnp.concatenate([value] + [from_rep(value, k) for k in range(1, n_rep)], axis=0)

    def exchange_parts(value):
        pieces = [column_part(value, r)]
        for k in range(1, n_rep):
            pieces.append(from_rep(column_part(value, (r - k + n_rep) % n_rep), k))
        return jnp.concatenate(pieces, axis=0)

    def rotate(value):
        result = []
        for j in range(n_in):
            cuts = [
                lax.dynamic_slice_in_dim(
                    value, (((zo + i) % n_out) * n_in + (yo + j) % n_in) * block, block, 1
                )
                for i in range(n_out)
            ]
            result.append(jnp.concatenate(cuts, axis=1))
        return jnp.concatenate(result, axis=1)

    def gather_rows(own):
        line = [own] + [from_outer(own, i) for i in range(1, n_out)]
        blocks = list(line)
        for j in range(1, n_in):
            blocks += [from_inner(b, j) for b in line]
        return jnp.concatenate(blocks, axis=0)

    down_all = gather_rows(column_part(down_weight, r).astype(BF))
    gate = exchange_parts(gate_pre).astype(F32)
    upper = exchange_parts(up_pre).astype(F32)
    ys = spread_tokens(rotate(cotangent))
    xs = spread_tokens(rotate(inputs))
    gs, us, ds = (column_part(s, r) for s in (gate_scale, up_scale, down_scale))

    sig = jax.nn.sigmoid(gate)
    act = gate * sig
    hidden = (act * upper).astype(BF)
    hidden_cot = jnp.dot(ys, down_all, preferred_element_type=F32) * ds
    gate_cot = (hidden_cot * upper * sig * (1.0 + gate * (1.0 - sig)) * gs).astype(BF)
    up_cot = (hidden_cot * act * us).astype(BF)
    both_cot = jnp.concatenate([gate_cot, up_cot], axis=1)

    dims = (((0,), (0,)), ((), ()))
    stretch = n_out * block

    def scattered(left, right, scale):
        def piece(j):
            value = lax.dot_general(
                left[:, j * stretch : (j + 1) * stretch], right, dims, preferred_element_type=F32
            )
            if scale is not None:
                value = value * scale
            return value

        arrived = []
        for j in range(1, n_in):
            arrived.append(from_inner(piece(j).astype(BF), n_in - j))
        total = piece(0)
        for value in arrived:
            total = total + value.astype(F32)
        own = total[:block]
        sent = total[block:].astype(BF)
        for i in range(1, n_out):
            own = own + from_outer(sent[(i - 1) * block : i * block], n_out - i).astype(F32)
        return lax.reduce_precision(own, 8, 7)

    def whole_columns(own):
        result = jnp.zeros((block, part * n_rep), F32)
        narrow = own.astype(BF)
        result = lax.dynamic_update_slice_in_dim(result, own, r * part, 1)
        for k in range(1, n_rep):
            value = from_rep(narrow, k).astype(F32)
            result = lax.dynamic_update_slice_in_dim(result, value, ((r + k) % n_rep) * part, 1)
        return result

    down_grad = whole_columns(scattered(ys, hidden, ds))
    gate_grad = whole_columns(scattered(xs, gate_cot, None))
    up_grad = whole_columns(scattered(xs, up_cot, None))

    both_rows = jnp.concatenate([column_part(gate_weight, r), column_part(up_weight, r)], axis=1)
    both_all = gather_rows(both_rows.astype(BF))
    partial = lax.dot_general(
        both_cot, both_all, (((1,), (1,)), ((), ())), preferred_element_type=F32
    ).astype(BF)
    back = []
    for z in range(n_out):
        for y in range(n_in):
            i = (z - zo + n_out) % n_out
            j = (y - yo + n_in) % n_in
            back.append(lax.dynamic_slice_in_dim(partial, (j * n_out + i) * block, block, 1))
    partial = jnp.concatenate(back, axis=1)
    share = width // n_tp
    total = lax.dynamic_slice_in_dim(partial, t * share, share, 1).astype(F32)
    for k in range(1, n_tp):
        target = (t - k + n_tp) % n_tp
        total = total + from_tp(
            lax.dynamic_slice_in_dim(partial, target * share, share, 1), k
        ).astype(F32)
    grad = total[:tokens]
    away = total[tokens:].astype(BF)
    for k in range(1, n_rep):
        grad = grad + from_rep(away[(k - 1) * tokens : k * tokens], n_rep - k).astype(F32)
    return (grad.astype(BF), gate_grad, up_grad, down_grad)


MESH = pl.DeviceIdType.MESH
ROWS = 32


def span(start, size):
    return pl.ds(pl.multiple_of(start, 16), size)


def whole_step(
    n_in,
    n_out,
    cot,
    inp,
    gate_in,
    up_in,
    quarters,
    scales_in,
    grads,
    shares,
    weights,
    gate,
    upper,
    ys,
    xs,
    hidden,
    own_down,
    own_up,
    away_down,
    passed,
    slots,
    scales,
    send_sems,
    recv_sems,
):
    x = lax.axis_index("rep")
    f = lax.axis_index("fs")
    c = lax.axis_index("tp")
    z, y = f // n_in, f % n_in
    home = c == y
    away = c != y
    tokens, width = cot.shape
    part = gate.shape[1]
    block = width // (n_in * n_out)
    half = width // 2
    last = n_out - 1

    def device(a, b, d, e):
        return (a, b * n_in + d, e)

    keys = {}
    sent = []

    def key(*name):
        return keys.setdefault(name, len(keys))

    def remote(source, target, name, where):
        k = key(*name)
        return pltpu.make_async_remote_copy(
            src_ref=source,
            dst_ref=target,
            send_sem=send_sems.at[k],
            recv_sem=recv_sems.at[k],
            device_id=where,
            device_id_type=MESH,
        )

    def send(when, source, target, name, where):
        @pl.when(when)
        def _():
            remote(source, target, name, where).start()

        sent.append((name, when, source, target, where))

    def arrive(when, target, name, where):
        @pl.when(when)
        def _():
            remote(target, target, name, where).wait_recv()

    def drain(chosen):
        rest = []
        for entry in sent:
            name, when, source, target, where = entry
            if not chosen(name):
                rest.append(entry)
                continue

            @pl.when(when)
            def _():
                remote(source, target, name, where).wait_send()

        sent[:] = rest

    def local(when, source, target, name, wait):
        @pl.when(when)
        def _():
            copy = pltpu.make_async_copy(source, target, recv_sems.at[key("local", *name)])
            if wait:
                copy.wait()
            else:
                copy.start()

    yes = x >= 0
    flipped = device(x, z, c, y)
    crossed = device(1 - x, z, c, y)
    over_x = device(1 - x, z, y, c)
    over_y = device(x, z, 1 - y, c)
    partner = device(x, z, y, 1 - c)
    ahead = device(x, jnp.minimum(z + 1, last), y, c)
    behind = device(x, jnp.maximum(z - 1, 0), y, c)

    barrier = pltpu.get_barrier_semaphore()
    for i in range(1, 8):
        other = device((x + i // 4) % 2, z, (y + (i // 2) % 2) % 2, (c + i % 2) % 2)
        pl.semaphore_signal(barrier, inc=1, device_id=other, device_id_type=MESH)

    @pl.when(z < last)
    def _():
        pl.semaphore_signal(barrier, inc=1, device_id=ahead, device_id_type=MESH)

    @pl.when(z > 0)
    def _():
        pl.semaphore_signal(barrier, inc=1, device_id=behind, device_id_type=MESH)

    pl.semaphore_wait(barrier, 7 + (z < last).astype(jnp.int32) + (z > 0).astype(jnp.int32))

    def weight_rows(w, at, side):
        return weights.at[w, span((at * n_in + side) * block, block)]

    def send_quarter(w):
        local(home, quarters.at[w], weight_rows(w, z, y), ("q", w), False)
        send(away, quarters.at[w], weight_rows(w, z, y), ("q", w), flipped)

    def wait_quarter(w):
        local(home, quarters.at[w], weight_rows(w, z, c), ("q", w), True)
        arrive(away, weight_rows(w, z, c), ("q", w), flipped)

    def send_near(index, source, target):
        rows = target.at[span(x * tokens, tokens)]
        local(home, source, rows, ("t", index), False)
        send(home, source, rows, ("tx", index), over_x)
        send(away, source, rows, ("ty", index), flipped)

    def forward_near(index, target):
        cut = tokens // 2
        far = target.at[span((1 - x) * tokens, tokens)]
        near = target.at[span(x * tokens, tokens)]
        arrive(home, far, ("tx", index), over_x)
        arrive(away, near, ("ty", index), flipped)
        low = target.at[span((1 - x) * tokens, cut)]
        high = target.at[span(x * tokens + cut, cut)]
        send(home, low, low, ("tl", index), over_y)
        send(away, high, high, ("th", index), over_x)

    def wait_tokens(index, source, target):
        cut = tokens // 2
        local(home, source, target.at[span(x * tokens, tokens)], ("t", index), True)
        arrive(away, target.at[span((1 - x) * tokens, cut)], ("tl", index), over_y)
        arrive(away, target.at[span((1 - x) * tokens + cut, cut)], ("th", index), over_x)

    def columns(source, p):
        return source.at[:, pl.ds(pl.multiple_of(p * part, 128), part)]

    def send_kept(index, source, target):
        rows = target.at[span(x * tokens, tokens)]
        local(home, columns(source, x), rows, ("ga", index), False)
        send(away, columns(source, x), rows, ("ga", index), flipped)

    def send_crossed(index, source, target):
        rows = target.at[span(x * tokens, tokens)]
        send(yes, columns(source, 1 - x), rows, ("gb", index), crossed)

    def wait_pre(index, source, target):
        near = target.at[span(x * tokens, tokens)]
        far = target.at[span((1 - x) * tokens, tokens)]
        local(home, columns(source, x), near, ("ga", index), True)
        arrive(away, near, ("ga", index), flipped)
        arrive(yes, far, ("gb", index), crossed)

    def share_block(w, step, side, at, when):
        rows = weight_rows(w, at, c)
        send(when, rows, rows, ("d", w, step, side), partner)

    def start_line(w):
        wait_quarter(w)
        rows = weight_rows(w, z, c)
        send(z < last, rows, rows, ("a", w, 1), ahead)
        send(z > 0, rows, rows, ("b", w, 1), behind)
        share_block(w, 0, 0, z, yes)

    def line_step(w, step):
        rows = weight_rows(w, jnp.maximum(z - step, 0), c)
        arrive(z >= step, rows, ("a", w, step), behind)
        if step < last:
            send((z >= step) & (z < last), rows, rows, ("a", w, step + 1), ahead)
        share_block(w, step, 1, jnp.maximum(z - step, 0), z >= step)
        rows = weight_rows(w, jnp.minimum(z + step, last), c)
        arrive(z + step <= last, rows, ("b", w, step), ahead)
        if step < last:
            send((z + step <= last) & (z > 0), rows, rows, ("b", w, step + 1), behind)
        share_block(w, step, 2, jnp.minimum(z + step, last), z + step <= last)

    def wait_shared(w):
        arrive(yes, weight_rows(w, z, 1 - c), ("d", w, 0, 0), partner)
        for step in range(1, n_out):
            arrive(
                z >= step,
                weight_rows(w, jnp.maximum(z - step, 0), 1 - c),
                ("d", w, step, 1),
                partner,
            )
            arrive(
                z + step <= last,
                weight_rows(w, jnp.minimum(z + step, last), 1 - c),
                ("d", w, step, 2),
                partner,
            )

    tiles = []
    start = 0
    while start < part:
        tiles.append((start, min(256, part - start)))
        start += 256
    pair = 2 * tokens
    tall = 256

    def make_hidden():
        def body(i, carry):
            rows = span(i * 64, 64)
            for at, size in tiles:
                g = gate[rows, at : at + size].astype(F32)
                u = upper[rows, at : at + size].astype(F32)
                hidden[rows, at : at + size] = (g * jax.nn.sigmoid(g) * u).astype(BF)
            return carry

        lax.fori_loop(0, pair // 64, body, 0)

    def make_cots(first, stop):
        def body(i, carry):
            rows = span(i * tall, tall)
            for at, size in tiles:
                cols = slice(at, at + size)
                value = jnp.dot(ys[rows, :], weights[0, :, cols], preferred_element_type=F32)
                value = value * scales[2:3, cols]
                g = gate[rows, cols].astype(F32)
                u = upper[rows, cols].astype(F32)
                sig = jax.nn.sigmoid(g)
                act = g * sig
                slope = value * u * sig * (1.0 + g * (1.0 - sig)) * scales[0:1, cols]
                gate[rows, cols] = slope.astype(BF)
                upper[rows, cols] = (value * act * scales[1:2, cols]).astype(BF)
            return carry

        lax.fori_loop(first, stop, body, 0)

    mine = (own_down, hidden, own_up)
    theirs = (away_down, weights.at[0, :half], weights.at[0, half:])

    def product(w, left, right):
        def into(target, side):
            def body(i, carry):
                at = pl.multiple_of((i * n_in + side) * block, 128)
                a = left[:, pl.ds(at, block)]
                for start, size in tiles:
                    cols = slice(start, start + size)
                    value = lax.dot_general(
                        a, right[:, cols], (((0,), (0,)), ((), ())), preferred_element_type=F32
                    )
                    if w == 0:
                        value = value * scales[2:3, cols]
                    target[span(i * block, block), cols] = value.astype(BF)
                return carry

            lax.fori_loop(0, n_out, body, 0)

        into(theirs[w], 1 - c)
        send(yes, theirs[w], passed.at[w], ("p", w), partner)
        into(mine[w], c)
        arrive(yes, passed.at[w], ("p", w), partner)

    def add(when, w, at, extra):
        @pl.when(when)
        def _():
            def body(i, carry):
                rows = span(at * block + i * ROWS, ROWS)
                value = mine[w][rows, :].astype(F32) + passed[w, rows, :].astype(F32)
                for slot in extra:
                    value = value + slots[w, slot, span(i * ROWS, ROWS), :].astype(F32)
                mine[w][rows, :] = value.astype(BF)
                return carry

            lax.fori_loop(0, block // ROWS, body, 0)

    def slot(side, step):
        return step - 1 if side == 0 or step == 1 else n_out - 3 + step

    def chain(w, step):
        def go(side, when, at, inner, where, back, letter):
            if step > 1:
                arrive(
                    when & inner,
                    slots.at[w, slot(side, step - 1)],
                    (letter, w, step - 1),
                    back,
                )
                add(when & inner, w, at, (slot(side, step - 1),))
            add(when & jnp.logical_not(inner), w, at, ())
            rows = mine[w].at[span(at * block, block)]
            send(when, rows, slots.at[w, slot(side, step)], (letter, w, step), where)

        go(0, z < step, jnp.minimum(z + n_out - step, last), z > 0, ahead, behind, "ra")
        go(
            1,
            z >= n_out - step,
            jnp.maximum(z - n_out + step, 0),
            z < last,
            behind,
            ahead,
            "rb",
        )

    def finish(w):
        arrive(z > 0, slots.at[w, slot(0, last)], ("ra", w, last), behind)
        arrive(z < last, slots.at[w, slot(1, last)], ("rb", w, last), ahead)
        both = (z > 0) & (z < last)
        add(both, w, z, (slot(0, last), slot(1, last)))
        add(z == 0, w, z, (slot(1, last),))
        add(z == last, w, z, (slot(0, last),))
        rows = mine[w].at[span(z * block, block)]
        target = grads.at[w, x]
        local(home, rows, target, ("f", w), False)
        send(away, rows, target, ("f", w), flipped)
        send(yes, rows, target, ("fc", w), crossed)

    def wait_finish(w):
        local(home, mine[w].at[span(z * block, block)], grads.at[w, x], ("f", w), True)
        arrive(away, grads.at[w, x], ("f", w), flipped)
        arrive(yes, grads.at[w, 1 - x], ("fc", w), crossed)

    def make_partial(first, stop):
        def body(i, carry):
            rows = span((i // (width // tall)) * tall, tall)
            cols = pl.multiple_of((i % (width // tall)) * tall, 128)
            dims = (((1,), (1,)), ((), ()))
            value = lax.dot_general(
                gate[rows, :],
                weights[1, pl.ds(cols, tall), :],
                dims,
                preferred_element_type=F32,
            )
            value = value + lax.dot_general(
                upper[rows, :],
                weights[2, pl.ds(cols, tall), :],
                dims,
                preferred_element_type=F32,
            )
            ys[rows, pl.ds(cols, tall)] = value.astype(BF)
            return carry

        lax.fori_loop(first, stop, body, 0)

    def partial_piece(a, e):
        share = width // n_in
        return ys.at[span(a * tokens, tokens), pl.ds(pl.multiple_of(e * share, 128), share)]

    def send_partial():
        target = shares.at[x * n_in + y]
        local(home, partial_piece(x, c), target, ("i",), False)
        for side in range(n_in):
            here = y == side
            send(here & away, partial_piece(x, c), target, ("i", 0, side), device(x, z, c, c))
            for n, (a, e) in enumerate(((x, 1 - c), (1 - x, c), (1 - x, 1 - c))):
                piece = partial_piece(a, e)
                send(here, piece, target, ("i", n + 1, side), device(a, z, c, e))

    def wait_partial():
        local(home, partial_piece(x, c), shares.at[x * n_in + y], ("i",), True)
        for side in range(n_in):
            near = shares.at[x * n_in + side]
            far = shares.at[(1 - x) * n_in + side]
            arrive(home & (y != side), near, ("i", 0, side), device(x, z, side, y))
            arrive(away, near, ("i", 1, side), device(x, z, side, y))
            arrive(home, far, ("i", 2, side), device(1 - x, z, side, y))
            arrive(away, far, ("i", 3, side), device(1 - x, z, side, y))

    local(home, scales_in, scales, ("s",), False)
    send(away, scales_in, scales, ("s",), flipped)
    send_quarter(0)
    send_near(0, cot, ys)
    send_quarter(1)
    send_kept(0, gate_in, gate)

    start_line(0)
    forward_near(0, ys)
    send_crossed(0, gate_in, gate)
    send_quarter(2)
    send_kept(1, up_in, upper)
    send_crossed(1, up_in, upper)
    send_near(1, inp, xs)
    line_step(0, 1)
    line_step(0, 2)
    start_line(1)
    for step in range(3, n_out):
        line_step(0, step)
    line_step(1, 1)
    start_line(2)
    line_step(1, 2)
    for step in range(3, n_out):
        line_step(1, step)

    local(home, scales_in, scales, ("s",), True)
    arrive(away, scales, ("s",), flipped)
    wait_tokens(0, cot, ys)
    wait_pre(0, gate_in, gate)
    wait_pre(1, up_in, upper)
    make_hidden()
    product(0, ys, hidden)
    chain(0, 1)
    line_step(2, 1)
    wait_shared(0)
    rows_of = pair // tall
    make_cots(0, rows_of // 2)
    chain(0, 2)
    line_step(2, 2)
    make_cots(rows_of // 2, rows_of)
    forward_near(1, xs)
    for step in range(3, n_out):
        chain(0, step)
        line_step(2, step)
    wait_tokens(1, inp, xs)
    drain(lambda name: name[:2] in (("a", 0), ("b", 0), ("d", 0)) or name == ("q", 0))
    product(1, xs, gate)
    chain(1, 1)
    finish(0)
    product(2, xs, upper)
    chain(1, 2)
    chain(2, 1)
    wait_shared(1)
    wait_shared(2)
    drain(lambda name: name in (("tl", 0), ("th", 0)))
    count = rows_of * (width // tall)
    make_partial(0, count // 2)
    for step in range(3, n_out):
        chain(1, step)
    make_partial(count // 2, count)
    send_partial()
    finish(1)
    for step in range(2, n_out):
        chain(2, step)
    finish(2)
    for w in range(3):
        wait_finish(w)
    wait_partial()
    drain(lambda name: True)


def shared(
    n_rep,
    n_fs,
    n_tp,
    inputs,
    cotangent,
    gate_pre,
    up_pre,
    gate_weight,
    up_weight,
    down_weight,
    gate_scale,
    up_scale,
    down_scale,
):
    n_in = n_tp
    n_out = n_fs // n_in
    tokens, width = inputs.shape
    block = width // n_fs
    part = gate_pre.shape[1] // n_rep
    half = width // 2
    x = lax.axis_index("rep")

    def column_part(value):
        return lax.dynamic_slice_in_dim(value, x * part, part, 1)

    quarters = jnp.stack(
        [column_part(v).astype(BF) for v in (down_weight, gate_weight, up_weight)]
    )
    scales = jnp.concatenate([gate_scale, up_scale, down_scale], axis=0)
    scales = jnp.pad(column_part(scales), ((0, 5), (0, 0)))
    n_sems = 128
    grads, shares = pl.pallas_call(
        functools.partial(whole_step, n_in, n_out),
        out_shape=(
            jax.ShapeDtypeStruct((3, n_rep, block, part), BF),
            jax.ShapeDtypeStruct((n_rep * n_in, tokens, width // n_tp), BF),
        ),
        in_specs=[pl.BlockSpec(memory_space=pltpu.HBM)] * 6,
        out_specs=(
            pl.BlockSpec(memory_space=pltpu.HBM),
            pl.BlockSpec(memory_space=pltpu.HBM),
        ),
        scratch_shapes=[
            pltpu.VMEM((3, width, part), BF),
            pltpu.VMEM((2 * tokens, part), BF),
            pltpu.VMEM((2 * tokens, part), BF),
            pltpu.VMEM((2 * tokens, width), BF),
            pltpu.VMEM((2 * tokens, width), BF),
            pltpu.VMEM((2 * tokens, part), BF),
            pltpu.VMEM((half, part), BF),
            pltpu.VMEM((half, part), BF),
            pltpu.VMEM((half, part), BF),
            pltpu.VMEM((3, half, part), BF),
            pltpu.VMEM((3, 2 * n_out - 3, block, part), BF),
            pltpu.VMEM((8, part), F32),
            pltpu.SemaphoreType.DMA((n_sems,)),
            pltpu.SemaphoreType.DMA((n_sems,)),
        ],
        compiler_params=pltpu.CompilerParams(
            collective_id=0, has_side_effects=True, vmem_limit_bytes=67043328
        ),
    )(cotangent, inputs, gate_pre, up_pre, quarters, scales)
    wide = [
        jnp.concatenate([grads[w, p] for p in range(n_rep)], axis=1).astype(F32)
        for w in range(3)
    ]
    grad = jnp.sum(shares.astype(F32), axis=0).astype(BF)
    return (grad, wide[1], wide[2], wide[0])


def fits(sizes, arrays):
    n_rep, n_fs, n_tp = sizes
    tokens, width = arrays[0].shape
    part = arrays[2].shape[1] // n_rep
    return (
        n_rep == 2
        and n_tp == 2
        and n_fs == 8
        and part % 128 == 0
        and width % (n_fs * 128) == 0
        and tokens % 256 == 0
    )


def local_step(sizes, *arrays):
    body = shared if fits(sizes, arrays) else local
    return body(*sizes, *arrays)


def solution(mesh):
    sizes = mesh.shape
    return jax.shard_map(
        functools.partial(local_step, (sizes["rep"], sizes["fs"], sizes["tp"])),
        mesh=mesh,
        in_specs=(
            P(("rep", "fs"), None),
            P(("rep", "fs"), None),
            P(("rep", "fs"), "tp"),
            P(("rep", "fs"), "tp"),
            P("fs", "tp"),
            P("fs", "tp"),
            P("fs", "tp"),
            P(None, "tp"),
            P(None, "tp"),
            P(None, "tp"),
        ),
        out_specs=(P(("rep", "fs"), "tp"), P("fs", "tp"), P("fs", "tp"), P("fs", "tp")),
        check_vma=False,
    )
```

```python
import functools

import jax
import jax.numpy as jnp
from jax import lax
from jax.experimental import pallas as pl
from jax.experimental.pallas import tpu as pltpu
from jax.sharding import PartitionSpec as P


BF = jnp.bfloat16
F32 = jnp.float32


def local(
    n_rep,
    n_fs,
    n_tp,
    inputs,
    cotangent,
    gate_pre,
    up_pre,
    gate_weight,
    up_weight,
    down_weight,
    gate_scale,
    up_scale,
    down_scale,
):
    n_out = 4 if n_fs % 4 == 0 else 1
    n_in = n_fs // n_out
    tokens = inputs.shape[0]
    width = inputs.shape[1]
    block = width // n_fs
    part = gate_pre.shape[1] // n_rep
    r = lax.axis_index("rep")
    f = lax.axis_index("fs")
    t = lax.axis_index("tp")
    zo, yo = f // n_in, f % n_in

    def from_rep(value, k):
        return lax.ppermute(value, "rep", [((i + k) % n_rep, i) for i in range(n_rep)])

    def from_tp(value, k):
        return lax.ppermute(value, "tp", [((i + k) % n_tp, i) for i in range(n_tp)])

    def from_outer(value, k):
        pairs = [
            (((z + k) % n_out) * n_in + y, z * n_in + y)
            for z in range(n_out)
            for y in range(n_in)
        ]
        return lax.ppermute(value, "fs", pairs)

    def from_inner(value, k):
        pairs = [
            (z * n_in + (y + k) % n_in, z * n_in + y)
            for z in range(n_out)
            for y in range(n_in)
        ]
        return lax.ppermute(value, "fs", pairs)

    def column_part(value, index):
        return lax.dynamic_slice_in_dim(value, index * part, part, 1)

    def spread_tokens(value):
        return jnp.concatenate([value] + [from_rep(value, k) for k in range(1, n_rep)], axis=0)

    def exchange_parts(value):
        pieces = [column_part(value, r)]
        for k in range(1, n_rep):
            pieces.append(from_rep(column_part(value, (r - k + n_rep) % n_rep), k))
        return jnp.concatenate(pieces, axis=0)

    def rotate(value):
        result = []
        for j in range(n_in):
            cuts = [
                lax.dynamic_slice_in_dim(
                    value, (((zo + i) % n_out) * n_in + (yo + j) % n_in) * block, block, 1
                )
                for i in range(n_out)
            ]
            result.append(jnp.concatenate(cuts, axis=1))
        return jnp.concatenate(result, axis=1)

    def gather_rows(own):
        line = [own] + [from_outer(own, i) for i in range(1, n_out)]
        blocks = list(line)
        for j in range(1, n_in):
            blocks += [from_inner(b, j) for b in line]
        return jnp.concatenate(blocks, axis=0)

    down_all = gather_rows(column_part(down_weight, r).astype(BF))
    gate = exchange_parts(gate_pre).astype(F32)
    upper = exchange_parts(up_pre).astype(F32)
    ys = spread_tokens(rotate(cotangent))
    xs = spread_tokens(rotate(inputs))
    gs, us, ds = (column_part(s, r) for s in (gate_scale, up_scale, down_scale))

    sig = jax.nn.sigmoid(gate)
    act = gate * sig
    hidden = (act * upper).astype(BF)
    hidden_cot = jnp.dot(ys, down_all, preferred_element_type=F32) * ds
    gate_cot = (hidden_cot * upper * sig * (1.0 + gate * (1.0 - sig)) * gs).astype(BF)
    up_cot = (hidden_cot * act * us).astype(BF)
    both_cot = jnp.concatenate([gate_cot, up_cot], axis=1)

    dims = (((0,), (0,)), ((), ()))
    stretch = n_out * block

    def scattered(left, right, scale):
        def piece(j):
            value = lax.dot_general(
                left[:, j * stretch : (j + 1) * stretch], right, dims, preferred_element_type=F32
            )
            if scale is not None:
                value = value * scale
            return value

        arrived = []
        for j in range(1, n_in):
            arrived.append(from_inner(piece(j).astype(BF), n_in - j))
        total = piece(0)
        for value in arrived:
            total = total + value.astype(F32)
        own = total[:block]
        sent = total[block:].astype(BF)
        for i in range(1, n_out):
            own = own + from_outer(sent[(i - 1) * block : i * block], n_out - i).astype(F32)
        return lax.reduce_precision(own, 8, 7)

    def whole_columns(own):
        result = jnp.zeros((block, part * n_rep), F32)
        narrow = own.astype(BF)
        result = lax.dynamic_update_slice_in_dim(result, own, r * part, 1)
        for k in range(1, n_rep):
            value = from_rep(narrow, k).astype(F32)
            result = lax.dynamic_update_slice_in_dim(result, value, ((r + k) % n_rep) * part, 1)
        return result

    down_grad = whole_columns(scattered(ys, hidden, ds))
    gate_grad = whole_columns(scattered(xs, gate_cot, None))
    up_grad = whole_columns(scattered(xs, up_cot, None))

    both_rows = jnp.concatenate([column_part(gate_weight, r), column_part(up_weight, r)], axis=1)
    both_all = gather_rows(both_rows.astype(BF))
    partial = lax.dot_general(
        both_cot, both_all, (((1,), (1,)), ((), ())), preferred_element_type=F32
    ).astype(BF)
    back = []
    for z in range(n_out):
        for y in range(n_in):
            i = (z - zo + n_out) % n_out
            j = (y - yo + n_in) % n_in
            back.append(lax.dynamic_slice_in_dim(partial, (j * n_out + i) * block, block, 1))
    partial = jnp.concatenate(back, axis=1)
    share = width // n_tp
    total = lax.dynamic_slice_in_dim(partial, t * share, share, 1).astype(F32)
    for k in range(1, n_tp):
        target = (t - k + n_tp) % n_tp
        total = total + from_tp(
            lax.dynamic_slice_in_dim(partial, target * share, share, 1), k
        ).astype(F32)
    grad = total[:tokens]
    away = total[tokens:].astype(BF)
    for k in range(1, n_rep):
        grad = grad + from_rep(away[(k - 1) * tokens : k * tokens], n_rep - k).astype(F32)
    return (grad.astype(BF), gate_grad, up_grad, down_grad)


MESH = pl.DeviceIdType.MESH
ROWS = 32


def span(start, size):
    return pl.ds(pl.multiple_of(start, 16), size)


def whole_step(
    n_in,
    n_out,
    cot,
    inp,
    gate_in,
    up_in,
    down_weight,
    gate_weight,
    up_weight,
    gate_factor,
    up_factor,
    down_factor,
    grads,
    shares,
    grad,
    weights,
    gate,
    upper,
    ys,
    xs,
    hidden,
    own_down,
    own_up,
    away_down,
    passed,
    slots,
    gate_scales,
    up_scales,
    down_scales,
    staged,
    send_sems,
    recv_sems,
):
    x = lax.axis_index("rep")
    f = lax.axis_index("fs")
    c = lax.axis_index("tp")
    z, y = f // n_in, f % n_in
    home = c == y
    away = c != y
    tokens, width = cot.shape
    part = gate.shape[1]
    block = width // (n_in * n_out)
    half = width // 2
    last = n_out - 1

    def device(a, b, d, e):
        return (a, b * n_in + d, e)

    keys = {}
    sent = []

    def key(*name):
        return keys.setdefault(name, len(keys))

    def remote(source, target, name, where):
        k = key(*name)
        return pltpu.make_async_remote_copy(
            src_ref=source,
            dst_ref=target,
            send_sem=send_sems.at[k],
            recv_sem=recv_sems.at[k],
            device_id=where,
            device_id_type=MESH,
        )

    def send(when, source, target, name, where):
        @pl.when(when)
        def _():
            remote(source, target, name, where).start()

        sent.append((name, when, source, target, where))

    def arrive(when, target, name, where):
        @pl.when(when)
        def _():
            remote(target, target, name, where).wait_recv()

    def drain(chosen):
        rest = []
        for entry in sent:
            name, when, source, target, where = entry
            if not chosen(name):
                rest.append(entry)
                continue

            @pl.when(when)
            def _():
                remote(source, target, name, where).wait_send()

        sent[:] = rest

    def local(when, source, target, name, wait):
        @pl.when(when)
        def _():
            copy = pltpu.make_async_copy(source, target, recv_sems.at[key("local", *name)])
            if wait:
                copy.wait()
            else:
                copy.start()

    yes = x >= 0
    stored = (down_weight, gate_weight, up_weight)
    factors = (
        (gate_factor, gate_scales),
        (up_factor, up_scales),
        (down_factor, down_scales),
    )
    flipped = device(x, z, c, y)
    crossed = device(1 - x, z, c, y)
    over_x = device(1 - x, z, y, c)
    over_y = device(x, z, 1 - y, c)
    partner = device(x, z, y, 1 - c)
    ahead = device(x, jnp.minimum(z + 1, last), y, c)
    behind = device(x, jnp.maximum(z - 1, 0), y, c)

    def load_stored(w):
        quarter = stored[w].at[:, pl.ds(pl.multiple_of(x * part, 128), part)]
        return pltpu.make_async_copy(quarter, staged, recv_sems.at[key("w", w)])

    def narrowed(w):
        return own_up.at[w * block : (w + 1) * block]

    def narrow(w):
        load_stored(w).wait()

        def into(target, base):
            def body(i, carry):
                rows = staged[span(i * ROWS, ROWS), :].astype(BF)
                target[span(base + i * ROWS, ROWS), :] = rows
                return carry

            lax.fori_loop(0, block // ROWS, body, 0)

        @pl.when(home)
        def _():
            into(weights.at[w], (z * n_in + c) * block)

        @pl.when(away)
        def _():
            into(own_up, w * block)

        if w < 2:
            load_stored(w + 1).start()

    load_stored(0).start()

    barrier = pltpu.get_barrier_semaphore()
    for i in range(1, 8):
        other = device((x + i // 4) % 2, z, (y + (i // 2) % 2) % 2, (c + i % 2) % 2)
        pl.semaphore_signal(barrier, inc=1, device_id=other, device_id_type=MESH)

    @pl.when(z < last)
    def _():
        pl.semaphore_signal(barrier, inc=1, device_id=ahead, device_id_type=MESH)

    @pl.when(z > 0)
    def _():
        pl.semaphore_signal(barrier, inc=1, device_id=behind, device_id_type=MESH)

    for w in range(3):
        narrow(w)

    pl.semaphore_wait(barrier, 7 + (z < last).astype(jnp.int32) + (z > 0).astype(jnp.int32))

    def weight_rows(w, at, side):
        return weights.at[w, span((at * n_in + side) * block, block)]

    def send_quarter(w):
        send(away, narrowed(w), weight_rows(w, z, y), ("q", w), flipped)

    def wait_quarter(w):
        arrive(away, weight_rows(w, z, c), ("q", w), flipped)

    cuts = (tokens // 8, tokens // 8 * 3)

    def piece(index, target, a, high):
        cut = cuts[index]
        if high:
            return target.at[span(a * tokens + cut, tokens - cut)]
        return target.at[span(a * tokens, cut)]

    def keep_near(index, source, target):
        local(home, source, target.at[span(x * tokens, tokens)], ("t", index), False)

    def near_over_x(when, index, source, target):
        where = device(1 - x, z, y, y)
        for high in (0, 1):
            rows = piece(index, target, x, high)
            send(when, piece(index, source, 0, high), rows, ("tx", index, high), where)

    def near_over_y(index, source, target):
        for high in (1, 0):
            rows = piece(index, target, x, high)
            send(away, piece(index, source, 0, high), rows, ("ty", index, high), flipped)

    def forward_low(index, target):
        low = piece(index, target, 1 - x, 0)
        arrive(home, low, ("tx", index, 0), over_x)
        send(home, low, low, ("tl", index), over_y)

    def forward_high(index, target):
        high = piece(index, target, x, 1)
        arrive(away, high, ("ty", index, 1), flipped)
        send(away, high, high, ("th", index), over_x)

    def wait_tokens(index, source, target):
        local(home, source, target.at[span(x * tokens, tokens)], ("t", index), True)
        arrive(home, piece(index, target, 1 - x, 1), ("tx", index, 1), over_x)
        arrive(away, piece(index, target, x, 0), ("ty", index, 0), flipped)
        arrive(away, piece(index, target, 1 - x, 0), ("tl", index), over_y)
        arrive(away, piece(index, target, 1 - x, 1), ("th", index), over_x)

    middle = (part // 128 + 1) // 2 * 128
    bounds = ((0, middle), (middle, part))

    def columns(source, p, h):
        low, high = bounds[h]
        return source.at[:, pl.ds(pl.multiple_of(p * part + low, 128), high - low)]

    def pre_rows(target, a, h):
        low, high = bounds[h]
        return target.at[span(a * tokens, tokens), low:high]

    def send_kept(index, h, source, target):
        rows = pre_rows(target, x, h)
        local(home, columns(source, x, h), rows, ("ga", index, h), False)
        send(away, columns(source, x, h), rows, ("ga", index, h), flipped)

    def send_crossed(when, which, index, h, source, target):
        rows = pre_rows(target, x, h)
        send(when, columns(source, 1 - x, h), rows, ("gb", index, h, which), crossed)

    def wait_pre(index, h, source, target):
        near = pre_rows(target, x, h)
        far = pre_rows(target, 1 - x, h)
        local(home, columns(source, x, h), near, ("ga", index, h), True)
        arrive(away, near, ("ga", index, h), flipped)
        arrive(home, far, ("gb", index, h, 0), over_x)
        arrive(away, far, ("gb", index, h, 1), crossed)

    def share_block(w, step, side, at, when):
        rows = weight_rows(w, at, c)
        send(when, rows, rows, ("d", w, step, side), partner)

    def start_line(w):
        wait_quarter(w)
        rows = weight_rows(w, z, c)
        send(z < last, rows, rows, ("a", w, 1), ahead)
        send(z > 0, rows, rows, ("b", w, 1), behind)
        share_block(w, 0, 0, z, yes)

    def line_step(w, step):
        rows = weight_rows(w, jnp.maximum(z - step, 0), c)
        arrive(z >= step, rows, ("a", w, step), behind)
        if step < last:
            send((z >= step) & (z < last), rows, rows, ("a", w, step + 1), ahead)
        share_block(w, step, 1, jnp.maximum(z - step, 0), z >= step)
        rows = weight_rows(w, jnp.minimum(z + step, last), c)
        arrive(z + step <= last, rows, ("b", w, step), ahead)
        if step < last:
            send((z + step <= last) & (z > 0), rows, rows, ("b", w, step + 1), behind)
        share_block(w, step, 2, jnp.minimum(z + step, last), z + step <= last)

    def wait_shared(w):
        arrive(yes, weight_rows(w, z, 1 - c), ("d", w, 0, 0), partner)
        for step in range(1, n_out):
            arrive(
                z >= step,
                weight_rows(w, jnp.maximum(z - step, 0), 1 - c),
                ("d", w, step, 1),
                partner,
            )
            arrive(
                z + step <= last,
                weight_rows(w, jnp.minimum(z + step, last), 1 - c),
                ("d", w, step, 2),
                partner,
            )

    def tiles(h):
        low, high = bounds[h]
        return [(at, min(256, high - at)) for at in range(low, high, 256)]

    pair = 2 * tokens
    tall = 256

    def make_hidden(h):
        def body(i, carry):
            rows = span(i * 64, 64)
            for at, size in tiles(h):
                g = gate[rows, at : at + size].astype(F32)
                u = upper[rows, at : at + size].astype(F32)
                hidden[rows, at : at + size] = (g * jax.nn.sigmoid(g) * u).astype(BF)
            return carry

        lax.fori_loop(0, pair // 64, body, 0)

    def make_cots(h):
        def body(i, carry):
            rows = span(i * tall, tall)
            for at, size in tiles(h):
                cols = slice(at, at + size)
                value = jnp.dot(ys[rows, :], weights[0, :, cols], preferred_element_type=F32)
                value = value * down_scales[:, cols]
                g = gate[rows, cols].astype(F32)
                u = upper[rows, cols].astype(F32)
                sig = jax.nn.sigmoid(g)
                act = g * sig
                slope = value * u * sig * (1.0 + g * (1.0 - sig)) * gate_scales[:, cols]
                gate[rows, cols] = slope.astype(BF)
                upper[rows, cols] = (value * act * up_scales[:, cols]).astype(BF)
            return carry

        lax.fori_loop(0, pair // tall, body, 0)

    mine = (own_down, hidden, own_up)
    theirs = (away_down, weights.at[0, :half], weights.at[0, half:])

    def product(w, h, left, right):
        low, high = bounds[h]


        def into(target, side):
            def body(i, carry):
                at = pl.multiple_of((i * n_in + side) * block, 128)
                a = left[:, pl.ds(at, block)]
                for start, size in tiles(h):
                    cols = slice(start, start + size)
                    value = lax.dot_general(
                        a, right[:, cols], (((0,), (0,)), ((), ())), preferred_element_type=F32
                    )
                    if w == 0:
                        value = value * down_scales[:, cols]
                    target[span(i * block, block), cols] = value.astype(BF)
                return carry

            lax.fori_loop(0, n_out, body, 0)

        into(theirs[w], 1 - c)
        landed = passed.at[w, :, low:high]
        send(yes, theirs[w].at[:, low:high], landed, ("p", w, h), partner)
        into(mine[w], c)
        arrive(yes, landed, ("p", w, h), partner)

    def add(when, w, h, at, extra):
        low, high = bounds[h]

        @pl.when(when)
        def _():
            def body(i, carry):
                rows = span(at * block + i * ROWS, ROWS)
                value = mine[w][rows, low:high].astype(F32)
                value = value + passed[w, rows, low:high].astype(F32)
                for n in extra:
                    more = slots[w, n, span(i * ROWS, ROWS), low:high]
                    value = value + more.astype(F32)
                mine[w][rows, low:high] = value.astype(BF)
                return carry

            lax.fori_loop(0, block // ROWS, body, 0)

    def slot(side, step):
        return step - 1 if side == 0 or step == 1 else n_out - 3 + step

    def landing(w, h, side, step):
        low, high = bounds[h]
        return slots.at[w, slot(side, step), :, low:high]

    def summed(w, h, at):
        low, high = bounds[h]
        return mine[w].at[span(at * block, block), low:high]

    ways = (
        (lambda step: jnp.minimum(z + n_out - step, last), ahead, behind),
        (lambda step: jnp.maximum(z - n_out + step, 0), behind, ahead),
    )

    def launch(w, h):
        for step in range(1, n_out):
            for side, when in ((0, z == 0), (1, z == last)):
                at, where, _ = ways[side]
                add(when, w, h, at(step), ())
                there = landing(w, h, side, step)
                send(when, summed(w, h, at(step)), there, ("r", side, w, h, step), where)

    def chain(w, h, step):
        for side, when in ((0, (z > 0) & (z < step)), (1, (z < last) & (z >= n_out - step))):
            at, where, back = ways[side]
            there = landing(w, h, side, step - 1)
            arrive(when, there, ("r", side, w, h, step - 1), back)
            add(when, w, h, at(step), (slot(side, step - 1),))
            there = landing(w, h, side, step)
            send(when, summed(w, h, at(step)), there, ("r", side, w, h, step), where)

    def finish(w, h):
        low, high = bounds[h]
        arrive(z > 0, landing(w, h, 0, last), ("r", 0, w, h, last), behind)
        arrive(z < last, landing(w, h, 1, last), ("r", 1, w, h, last), ahead)
        both = (z > 0) & (z < last)
        add(both, w, h, z, (slot(0, last), slot(1, last)))
        add(z == 0, w, h, z, (slot(1, last),))
        add(z == last, w, h, z, (slot(0, last),))
        rows = summed(w, h, z)
        target = grads.at[w, x, :, low:high]
        local(home, rows, target, ("f", w, h), False)
        send(away, rows, target, ("f", w, h), flipped)
        send(home, rows, target, ("fc", w, h), over_x)
        if (w, h) == final:
            send(away, rows, target, ("fd", w, h), crossed)

    final = (2, 1)

    def pass_on(w, h):
        low, high = bounds[h]
        target = grads.at[w, x, :, low:high]
        arrive(away, target, ("f", w, h), flipped)
        send(away, target, target, ("fd", w, h), over_x)

    def wait_finish(w, h):
        low, high = bounds[h]
        target = grads.at[w, x, :, low:high]
        other = grads.at[w, 1 - x, :, low:high]
        local(home, summed(w, h, z), target, ("f", w, h), True)
        arrive(home, other, ("fc", w, h), over_x)
        if (w, h) == final:
            arrive(away, target, ("f", w, h), flipped)
        arrive(away, other, ("fd", w, h), crossed if (w, h) == final else over_x)

    def make_partial(a):
        def body(i, carry):
            rows = span(a * tokens + (i // (width // tall)) * tall, tall)
            cols = pl.multiple_of((i % (width // tall)) * tall, 128)
            dims = (((1,), (1,)), ((), ()))
            value = lax.dot_general(
                gate[rows, :],
                weights[1, pl.ds(cols, tall), :],
                dims,
                preferred_element_type=F32,
            )
            value = value + lax.dot_general(
                upper[rows, :],
                weights[2, pl.ds(cols, tall), :],
                dims,
                preferred_element_type=F32,
            )
            ys[rows, pl.ds(cols, tall)] = value.astype(BF)
            return carry

        lax.fori_loop(0, (tokens // tall) * (width // tall), body, 0)

    def partial_piece(a, e):
        share = width // n_in
        return ys.at[span(a * tokens, tokens), pl.ds(pl.multiple_of(e * share, 128), share)]

    def send_partial(a, first):
        target = shares.at[x * n_in + y]
        near, far = device(a, z, c, c), device(a, z, c, 1 - c)
        if first == 0:
            local(home, partial_piece(a, c), target, ("i",), False)
        for side in range(n_in):
            here = (y == side) & (away if first == 0 else yes)
            send(here, partial_piece(a, c), target, ("i", first, side), near)
            send(y == side, partial_piece(a, 1 - c), target, ("i", first + 1, side), far)

    def wait_partial():
        local(home, partial_piece(x, c), shares.at[x * n_in + y], ("i",), True)
        for side in range(n_in):
            near = shares.at[x * n_in + side]
            far = shares.at[(1 - x) * n_in + side]
            arrive(home & (y != side), near, ("i", 0, side), device(x, z, side, y))
            arrive(away, near, ("i", 1, side), device(x, z, side, y))
            arrive(home, far, ("i", 2, side), device(1 - x, z, side, y))
            arrive(away, far, ("i", 3, side), device(1 - x, z, side, y))

    def add_partial():
        wide = width // n_in
        places = [(a, d) for a in range(2) for d in range(n_in)]

        def load(a, d):
            there = xs.at[span(a * tokens, tokens), d * wide : (d + 1) * wide]
            k = recv_sems.at[key("load", a, d)]
            return pltpu.make_async_copy(shares.at[a * n_in + d], there, k)

        for place in places:
            load(*place).start()
        for place in places:
            load(*place).wait()

        def body(i, carry):
            value = None
            for a, d in places:
                rows = span(a * tokens + i * ROWS, ROWS)
                more = xs[rows, d * wide : (d + 1) * wide].astype(F32)
                value = more if value is None else value + more
            xs[span(i * ROWS, ROWS), :wide] = value.astype(BF)
            return carry

        lax.fori_loop(0, tokens // ROWS, body, 0)
        out = pltpu.make_async_copy(
            xs.at[span(0, tokens), :wide], grad, recv_sems.at[key("out")]
        )
        out.start()
        out.wait()

    def factor(n):
        return factors[n][0].at[:, pl.ds(pl.multiple_of(x * part, 128), part)]

    send_quarter(0)
    keep_near(0, cot, ys)
    near_over_x(home, 0, cot, ys)
    near_over_y(0, cot, ys)
    send_quarter(1)
    for n in range(3):
        local(home, factor(n), factors[n][1], ("s", n), False)
        send(away, factor(n), factors[n][1], ("s", n), flipped)
    send_kept(0, 0, gate_in, gate)
    send_kept(1, 0, up_in, upper)
    send_crossed(home, 0, 0, 0, gate_in, gate)
    send_crossed(home, 0, 1, 0, up_in, upper)
    keep_near(1, inp, xs)

    start_line(0)
    line_step(0, 1)
    forward_low(0, ys)
    forward_high(0, ys)
    send_crossed(away, 1, 0, 0, gate_in, gate)
    send_crossed(away, 1, 1, 0, up_in, upper)
    send_quarter(2)
    near_over_x(away, 1, inp, xs)
    near_over_y(1, inp, xs)
    line_step(0, 2)
    start_line(1)
    for step in range(3, n_out):
        line_step(0, step)
    line_step(1, 1)

    for n in range(3):
        local(home, factor(n), factors[n][1], ("s", n), True)
        arrive(away, factors[n][1], ("s", n), flipped)
    wait_tokens(0, cot, ys)
    wait_pre(0, 0, gate_in, gate)
    wait_pre(1, 0, up_in, upper)
    make_hidden(0)
    product(0, 0, ys, hidden)
    launch(0, 0)
    line_step(1, 2)
    start_line(2)
    wait_shared(0)
    drain(lambda name: name[0] == "q" or name[:2] in (("a", 0), ("b", 0), ("d", 0)))
    make_cots(0)
    forward_low(1, xs)
    chain(0, 0, 2)
    forward_high(1, xs)
    send_kept(0, 1, gate_in, gate)
    send_kept(1, 1, up_in, upper)
    for step in range(3, n_out):
        line_step(1, step)
    send_crossed(away, 1, 0, 1, gate_in, gate)
    send_crossed(away, 1, 1, 1, up_in, upper)
    for step in range(3, n_out):
        chain(0, 0, step)
    line_step(2, 1)
    wait_tokens(1, inp, xs)
    send_crossed(home, 0, 0, 1, gate_in, gate)
    send_crossed(home, 0, 1, 1, up_in, upper)
    product(1, 0, xs, gate)
    launch(1, 0)
    product(2, 0, xs, upper)
    launch(2, 0)
    line_step(2, 2)
    finish(0, 0)
    chain(1, 0, 2)

    wait_pre(0, 1, gate_in, gate)
    wait_pre(1, 1, up_in, upper)
    make_hidden(1)
    product(0, 1, ys, hidden)
    launch(0, 1)
    for step in range(3, n_out):
        chain(1, 0, step)
        line_step(2, step)
    make_cots(1)
    chain(2, 0, 2)
    wait_shared(1)
    wait_shared(2)
    drain(lambda name: name in (("tl", 0), ("th", 0)))
    pass_on(0, 0)
    make_partial(1 - x)
    send_partial(1 - x, 2)
    finish(1, 0)
    for step in range(3, n_out):
        chain(2, 0, step)
    make_partial(x)
    send_partial(x, 0)
    product(1, 1, xs, gate)
    launch(1, 1)
    pass_on(1, 0)
    chain(0, 1, 2)
    finish(2, 0)
    product(2, 1, xs, upper)
    launch(2, 1)
    for step in range(3, n_out):
        chain(0, 1, step)
    chain(1, 1, 2)
    finish(0, 1)
    for step in range(3, n_out):
        chain(1, 1, step)
    chain(2, 1, 2)
    finish(1, 1)
    pass_on(2, 0)
    for step in range(3, n_out):
        chain(2, 1, step)
    pass_on(0, 1)
    finish(2, 1)
    pass_on(1, 1)
    wait_partial()
    drain(lambda name: name in (("tl", 1), ("th", 1)))
    add_partial()
    for h in range(2):
        for w in range(3):
            wait_finish(w, h)
    drain(lambda name: True)


def shared(
    n_rep,
    n_fs,
    n_tp,
    inputs,
    cotangent,
    gate_pre,
    up_pre,
    gate_weight,
    up_weight,
    down_weight,
    gate_scale,
    up_scale,
    down_scale,
):
    n_in = n_tp
    n_out = n_fs // n_in
    tokens, width = inputs.shape
    block = width // n_fs
    part = gate_pre.shape[1] // n_rep
    half = width // 2
    x = lax.axis_index("rep")

    n_sems = 192
    grads, _, grad = pl.pallas_call(
        functools.partial(whole_step, n_in, n_out),
        out_shape=(
            jax.ShapeDtypeStruct((3, n_rep, block, part), BF),
            jax.ShapeDtypeStruct((n_rep * n_in, tokens, width // n_tp), BF),
            jax.ShapeDtypeStruct((tokens, width // n_tp), BF),
        ),
        in_specs=[pl.BlockSpec(memory_space=pltpu.HBM)] * 10,
        out_specs=(
            pl.BlockSpec(memory_space=pltpu.HBM),
            pl.BlockSpec(memory_space=pltpu.HBM),
            pl.BlockSpec(memory_space=pltpu.HBM),
        ),
        scratch_shapes=[
            pltpu.VMEM((3, width, part), BF),
            pltpu.VMEM((2 * tokens, part), BF),
            pltpu.VMEM((2 * tokens, part), BF),
            pltpu.VMEM((2 * tokens, width), BF),
            pltpu.VMEM((2 * tokens, width), BF),
            pltpu.VMEM((2 * tokens, part), BF),
            pltpu.VMEM((half, part), BF),
            pltpu.VMEM((half, part), BF),
            pltpu.VMEM((half, part), BF),
            pltpu.VMEM((3, half, part), BF),
            pltpu.VMEM((3, 2 * n_out - 3, block, part), BF),
            pltpu.VMEM((1, part), F32),
            pltpu.VMEM((1, part), F32),
            pltpu.VMEM((1, part), F32),
            pltpu.VMEM((block, part), F32),
            pltpu.SemaphoreType.DMA((n_sems,)),
            pltpu.SemaphoreType.DMA((n_sems,)),
        ],
        compiler_params=pltpu.CompilerParams(
            collective_id=0, has_side_effects=True, vmem_limit_bytes=67043328
        ),
    )(
        cotangent,
        inputs,
        gate_pre,
        up_pre,
        down_weight,
        gate_weight,
        up_weight,
        gate_scale,
        up_scale,
        down_scale,
    )
    wide = [
        jnp.concatenate([grads[w, p] for p in range(n_rep)], axis=1).astype(F32)
        for w in range(3)
    ]
    return (grad, wide[1], wide[2], wide[0])


def fits(sizes, arrays):
    n_rep, n_fs, n_tp = sizes
    tokens, width = arrays[0].shape
    part = arrays[2].shape[1] // n_rep
    return (
        n_rep == 2
        and n_tp == 2
        and n_fs == 8
        and part % 128 == 0
        and width % (n_fs * 128) == 0
        and tokens % 256 == 0
    )


def local_step(sizes, *arrays):
    body = shared if fits(sizes, arrays) else local
    return body(*sizes, *arrays)


def solution(mesh):
    sizes = mesh.shape
    return jax.shard_map(
        functools.partial(local_step, (sizes["rep"], sizes["fs"], sizes["tp"])),
        mesh=mesh,
        in_specs=(
            P(("rep", "fs"), None),
            P(("rep", "fs"), None),
            P(("rep", "fs"), "tp"),
            P(("rep", "fs"), "tp"),
            P("fs", "tp"),
            P("fs", "tp"),
            P("fs", "tp"),
            P(None, "tp"),
            P(None, "tp"),
            P(None, "tp"),
        ),
        out_specs=(P(("rep", "fs"), "tp"), P("fs", "tp"), P("fs", "tp"), P("fs", "tp")),
        check_vma=False,
    )
```

```python
import functools

import jax
import jax.numpy as jnp
from jax import lax
from jax.experimental import pallas as pl
from jax.experimental.pallas import tpu as pltpu
from jax.sharding import PartitionSpec as P


BF = jnp.bfloat16
F32 = jnp.float32


def local(
    n_rep,
    n_fs,
    n_tp,
    inputs,
    cotangent,
    gate_pre,
    up_pre,
    gate_weight,
    up_weight,
    down_weight,
    gate_scale,
    up_scale,
    down_scale,
):
    n_out = 4 if n_fs % 4 == 0 else 1
    n_in = n_fs // n_out
    tokens = inputs.shape[0]
    width = inputs.shape[1]
    block = width // n_fs
    part = gate_pre.shape[1] // n_rep
    r = lax.axis_index("rep")
    f = lax.axis_index("fs")
    t = lax.axis_index("tp")
    zo, yo = f // n_in, f % n_in

    def from_rep(value, k):
        return lax.ppermute(value, "rep", [((i + k) % n_rep, i) for i in range(n_rep)])

    def from_tp(value, k):
        return lax.ppermute(value, "tp", [((i + k) % n_tp, i) for i in range(n_tp)])

    def from_outer(value, k):
        pairs = [
            (((z + k) % n_out) * n_in + y, z * n_in + y)
            for z in range(n_out)
            for y in range(n_in)
        ]
        return lax.ppermute(value, "fs", pairs)

    def from_inner(value, k):
        pairs = [
            (z * n_in + (y + k) % n_in, z * n_in + y)
            for z in range(n_out)
            for y in range(n_in)
        ]
        return lax.ppermute(value, "fs", pairs)

    def column_part(value, index):
        return lax.dynamic_slice_in_dim(value, index * part, part, 1)

    def spread_tokens(value):
        return jnp.concatenate([value] + [from_rep(value, k) for k in range(1, n_rep)], axis=0)

    def exchange_parts(value):
        pieces = [column_part(value, r)]
        for k in range(1, n_rep):
            pieces.append(from_rep(column_part(value, (r - k + n_rep) % n_rep), k))
        return jnp.concatenate(pieces, axis=0)

    def rotate(value):
        result = []
        for j in range(n_in):
            cuts = [
                lax.dynamic_slice_in_dim(
                    value, (((zo + i) % n_out) * n_in + (yo + j) % n_in) * block, block, 1
                )
                for i in range(n_out)
            ]
            result.append(jnp.concatenate(cuts, axis=1))
        return jnp.concatenate(result, axis=1)

    def gather_rows(own):
        line = [own] + [from_outer(own, i) for i in range(1, n_out)]
        blocks = list(line)
        for j in range(1, n_in):
            blocks += [from_inner(b, j) for b in line]
        return jnp.concatenate(blocks, axis=0)

    down_all = gather_rows(column_part(down_weight, r).astype(BF))
    gate = exchange_parts(gate_pre).astype(F32)
    upper = exchange_parts(up_pre).astype(F32)
    ys = spread_tokens(rotate(cotangent))
    xs = spread_tokens(rotate(inputs))
    gs, us, ds = (column_part(s, r) for s in (gate_scale, up_scale, down_scale))

    sig = jax.nn.sigmoid(gate)
    act = gate * sig
    hidden = (act * upper).astype(BF)
    hidden_cot = jnp.dot(ys, down_all, preferred_element_type=F32) * ds
    gate_cot = (hidden_cot * upper * sig * (1.0 + gate * (1.0 - sig)) * gs).astype(BF)
    up_cot = (hidden_cot * act * us).astype(BF)
    both_cot = jnp.concatenate([gate_cot, up_cot], axis=1)

    dims = (((0,), (0,)), ((), ()))
    stretch = n_out * block

    def scattered(left, right, scale):
        def piece(j):
            value = lax.dot_general(
                left[:, j * stretch : (j + 1) * stretch], right, dims, preferred_element_type=F32
            )
            if scale is not None:
                value = value * scale
            return value

        arrived = []
        for j in range(1, n_in):
            arrived.append(from_inner(piece(j).astype(BF), n_in - j))
        total = piece(0)
        for value in arrived:
            total = total + value.astype(F32)
        own = total[:block]
        sent = total[block:].astype(BF)
        for i in range(1, n_out):
            own = own + from_outer(sent[(i - 1) * block : i * block], n_out - i).astype(F32)
        return lax.reduce_precision(own, 8, 7)

    def whole_columns(own):
        result = jnp.zeros((block, part * n_rep), F32)
        narrow = own.astype(BF)
        result = lax.dynamic_update_slice_in_dim(result, own, r * part, 1)
        for k in range(1, n_rep):
            value = from_rep(narrow, k).astype(F32)
            result = lax.dynamic_update_slice_in_dim(result, value, ((r + k) % n_rep) * part, 1)
        return result

    down_grad = whole_columns(scattered(ys, hidden, ds))
    gate_grad = whole_columns(scattered(xs, gate_cot, None))
    up_grad = whole_columns(scattered(xs, up_cot, None))

    both_rows = jnp.concatenate([column_part(gate_weight, r), column_part(up_weight, r)], axis=1)
    both_all = gather_rows(both_rows.astype(BF))
    partial = lax.dot_general(
        both_cot, both_all, (((1,), (1,)), ((), ())), preferred_element_type=F32
    ).astype(BF)
    back = []
    for z in range(n_out):
        for y in range(n_in):
            i = (z - zo + n_out) % n_out
            j = (y - yo + n_in) % n_in
            back.append(lax.dynamic_slice_in_dim(partial, (j * n_out + i) * block, block, 1))
    partial = jnp.concatenate(back, axis=1)
    share = width // n_tp
    total = lax.dynamic_slice_in_dim(partial, t * share, share, 1).astype(F32)
    for k in range(1, n_tp):
        target = (t - k + n_tp) % n_tp
        total = total + from_tp(
            lax.dynamic_slice_in_dim(partial, target * share, share, 1), k
        ).astype(F32)
    grad = total[:tokens]
    away = total[tokens:].astype(BF)
    for k in range(1, n_rep):
        grad = grad + from_rep(away[(k - 1) * tokens : k * tokens], n_rep - k).astype(F32)
    return (grad.astype(BF), gate_grad, up_grad, down_grad)


MESH = pl.DeviceIdType.MESH
ROWS = 32


def span(start, size):
    return pl.ds(pl.multiple_of(start, 16), size)


def whole_step(
    n_in,
    n_out,
    cot,
    inp,
    gate_in,
    up_in,
    down_weight,
    gate_weight,
    up_weight,
    gate_factor,
    up_factor,
    down_factor,
    grads,
    shares,
    grad,
    weights,
    gate,
    upper,
    ys,
    xs,
    hidden,
    own_down,
    own_up,
    away_down,
    passed,
    slots,
    gate_scales,
    up_scales,
    down_scales,
    staged,
    send_sems,
    recv_sems,
):
    x = lax.axis_index("rep")
    f = lax.axis_index("fs")
    c = lax.axis_index("tp")
    z, y = f // n_in, f % n_in
    home = c == y
    away = c != y
    tokens, width = cot.shape
    part = gate.shape[1]
    block = width // (n_in * n_out)
    half = width // 2
    last = n_out - 1

    def device(a, b, d, e):
        return (a, b * n_in + d, e)

    keys = {}
    sent = []

    def key(*name):
        return keys.setdefault(name, len(keys))

    def remote(source, target, name, where):
        k = key(*name)
        return pltpu.make_async_remote_copy(
            src_ref=source,
            dst_ref=target,
            send_sem=send_sems.at[k],
            recv_sem=recv_sems.at[k],
            device_id=where,
            device_id_type=MESH,
        )

    def send(when, source, target, name, where):
        @pl.when(when)
        def _():
            remote(source, target, name, where).start()

        sent.append((name, when, source, target, where))

    def arrive(when, target, name, where):
        @pl.when(when)
        def _():
            remote(target, target, name, where).wait_recv()

    def drain(chosen):
        rest = []
        for entry in sent:
            name, when, source, target, where = entry
            if not chosen(name):
                rest.append(entry)
                continue

            @pl.when(when)
            def _():
                remote(source, target, name, where).wait_send()

        sent[:] = rest

    def local(when, source, target, name, wait):
        @pl.when(when)
        def _():
            copy = pltpu.make_async_copy(source, target, recv_sems.at[key("local", *name)])
            if wait:
                copy.wait()
            else:
                copy.start()

    yes = x >= 0
    stored = (down_weight, gate_weight, up_weight)
    factors = (
        (gate_factor, gate_scales),
        (up_factor, up_scales),
        (down_factor, down_scales),
    )
    flipped = device(x, z, c, y)
    crossed = device(1 - x, z, c, y)
    over_x = device(1 - x, z, y, c)
    over_y = device(x, z, 1 - y, c)
    partner = device(x, z, y, 1 - c)
    ahead = device(x, jnp.minimum(z + 1, last), y, c)
    behind = device(x, jnp.maximum(z - 1, 0), y, c)

    def load_stored(w):
        quarter = stored[w].at[:, pl.ds(pl.multiple_of(x * part, 128), part)]
        return pltpu.make_async_copy(quarter, staged, recv_sems.at[key("w", w)])

    def narrowed(w):
        return own_up.at[w * block : (w + 1) * block]

    def narrow(w):
        load_stored(w).wait()

        def into(target, base):
            def body(i, carry):
                rows = staged[span(i * ROWS, ROWS), :].astype(BF)
                target[span(base + i * ROWS, ROWS), :] = rows
                return carry

            lax.fori_loop(0, block // ROWS, body, 0)

        @pl.when(home)
        def _():
            into(weights.at[w], (z * n_in + c) * block)

        @pl.when(away)
        def _():
            into(own_up, w * block)

        if w < 2:
            load_stored(w + 1).start()

    load_stored(0).start()

    barrier = pltpu.get_barrier_semaphore()
    for i in range(1, 8):
        other = device((x + i // 4) % 2, z, (y + (i // 2) % 2) % 2, (c + i % 2) % 2)
        pl.semaphore_signal(barrier, inc=1, device_id=other, device_id_type=MESH)

    @pl.when(z < last)
    def _():
        pl.semaphore_signal(barrier, inc=1, device_id=ahead, device_id_type=MESH)

    @pl.when(z > 0)
    def _():
        pl.semaphore_signal(barrier, inc=1, device_id=behind, device_id_type=MESH)

    narrow(0)
    pl.semaphore_wait(barrier, 7 + (z < last).astype(jnp.int32) + (z > 0).astype(jnp.int32))

    def weight_rows(w, at, side):
        return weights.at[w, span((at * n_in + side) * block, block)]

    def send_quarter(w):
        send(away, narrowed(w), weight_rows(w, z, y), ("q", w), flipped)

    def wait_quarter(w):
        arrive(away, weight_rows(w, z, c), ("q", w), flipped)

    cuts = (tokens // 8, tokens // 8 * 3)

    def piece(index, target, a, high):
        cut = cuts[index]
        if high:
            return target.at[span(a * tokens + cut, tokens - cut)]
        return target.at[span(a * tokens, cut)]

    def keep_near(index, source, target):
        local(home, source, target.at[span(x * tokens, tokens)], ("t", index), False)

    def near_over_x(when, index, source, target):
        where = device(1 - x, z, y, y)
        for high in (0, 1):
            rows = piece(index, target, x, high)
            send(when, piece(index, source, 0, high), rows, ("tx", index, high), where)

    def near_over_y(index, source, target):
        for high in (1, 0):
            rows = piece(index, target, x, high)
            send(away, piece(index, source, 0, high), rows, ("ty", index, high), flipped)

    def forward_low(index, target):
        low = piece(index, target, 1 - x, 0)
        arrive(home, low, ("tx", index, 0), over_x)
        send(home, low, low, ("tl", index), over_y)

    def forward_high(index, target):
        high = piece(index, target, x, 1)
        arrive(away, high, ("ty", index, 1), flipped)
        send(away, high, high, ("th", index), over_x)

    def wait_tokens(index, source, target):
        local(home, source, target.at[span(x * tokens, tokens)], ("t", index), True)
        arrive(home, piece(index, target, 1 - x, 1), ("tx", index, 1), over_x)
        arrive(away, piece(index, target, x, 0), ("ty", index, 0), flipped)
        arrive(away, piece(index, target, 1 - x, 0), ("tl", index), over_y)
        arrive(away, piece(index, target, 1 - x, 1), ("th", index), over_x)

    middle = (part // 128 + 1) // 2 * 128
    bounds = ((0, middle), (middle, part))

    def columns(source, p, h):
        low, high = bounds[h]
        return source.at[:, pl.ds(pl.multiple_of(p * part + low, 128), high - low)]

    def pre_rows(target, a, h):
        low, high = bounds[h]
        return target.at[span(a * tokens, tokens), low:high]

    def send_kept(index, h, source, target):
        rows = pre_rows(target, x, h)
        local(home, columns(source, x, h), rows, ("ga", index, h), False)
        send(away, columns(source, x, h), rows, ("ga", index, h), flipped)

    def send_crossed(when, which, index, h, source, target):
        rows = pre_rows(target, x, h)
        send(when, columns(source, 1 - x, h), rows, ("gb", index, h, which), crossed)

    def wait_pre(index, h, source, target):
        near = pre_rows(target, x, h)
        far = pre_rows(target, 1 - x, h)
        local(home, columns(source, x, h), near, ("ga", index, h), True)
        arrive(away, near, ("ga", index, h), flipped)
        arrive(home, far, ("gb", index, h, 0), over_x)
        arrive(away, far, ("gb", index, h, 1), crossed)

    def share_block(w, step, side, at, when):
        rows = weight_rows(w, at, c)
        send(when, rows, rows, ("d", w, step, side), partner)

    def start_line(w):
        wait_quarter(w)
        rows = weight_rows(w, z, c)
        send(z < last, rows, rows, ("a", w, 1), ahead)
        send(z > 0, rows, rows, ("b", w, 1), behind)
        share_block(w, 0, 0, z, yes)

    def line_step(w, step):
        rows = weight_rows(w, jnp.maximum(z - step, 0), c)
        arrive(z >= step, rows, ("a", w, step), behind)
        if step < last:
            send((z >= step) & (z < last), rows, rows, ("a", w, step + 1), ahead)
        share_block(w, step, 1, jnp.maximum(z - step, 0), z >= step)
        rows = weight_rows(w, jnp.minimum(z + step, last), c)
        arrive(z + step <= last, rows, ("b", w, step), ahead)
        if step < last:
            send((z + step <= last) & (z > 0), rows, rows, ("b", w, step + 1), behind)
        share_block(w, step, 2, jnp.minimum(z + step, last), z + step <= last)

    def wait_shared(w):
        arrive(yes, weight_rows(w, z, 1 - c), ("d", w, 0, 0), partner)
        for step in range(1, n_out):
            arrive(
                z >= step,
                weight_rows(w, jnp.maximum(z - step, 0), 1 - c),
                ("d", w, step, 1),
                partner,
            )
            arrive(
                z + step <= last,
                weight_rows(w, jnp.minimum(z + step, last), 1 - c),
                ("d", w, step, 2),
                partner,
            )

    def tiles(h):
        low, high = bounds[h]
        return [(at, min(256, high - at)) for at in range(low, high, 256)]

    pair = 2 * tokens
    tall = 256

    def make_hidden(h):
        def body(i, carry):
            rows = span(i * 64, 64)
            for at, size in tiles(h):
                g = gate[rows, at : at + size].astype(F32)
                u = upper[rows, at : at + size].astype(F32)
                hidden[rows, at : at + size] = (g * jax.nn.sigmoid(g) * u).astype(BF)
            return carry

        lax.fori_loop(0, pair // 64, body, 0)

    def make_cots(h):
        def body(i, carry):
            rows = span(i * tall, tall)
            for at, size in tiles(h):
                cols = slice(at, at + size)
                value = jnp.dot(ys[rows, :], weights[0, :, cols], preferred_element_type=F32)
                value = value * down_scales[:, cols]
                g = gate[rows, cols].astype(F32)
                u = upper[rows, cols].astype(F32)
                sig = jax.nn.sigmoid(g)
                act = g * sig
                slope = value * u * sig * (1.0 + g * (1.0 - sig)) * gate_scales[:, cols]
                gate[rows, cols] = slope.astype(BF)
                upper[rows, cols] = (value * act * up_scales[:, cols]).astype(BF)
            return carry

        lax.fori_loop(0, pair // tall, body, 0)

    mine = (own_down, hidden, own_up)
    theirs = (away_down, weights.at[0, :half], weights.at[0, half:])

    def product(w, h, left, right):
        low, high = bounds[h]


        def into(target, side):
            def body(i, carry):
                at = pl.multiple_of((i * n_in + side) * block, 128)
                a = left[:, pl.ds(at, block)]
                for start, size in tiles(h):
                    cols = slice(start, start + size)
                    value = lax.dot_general(
                        a, right[:, cols], (((0,), (0,)), ((), ())), preferred_element_type=F32
                    )
                    if w == 0:
                        value = value * down_scales[:, cols]
                    target[span(i * block, block), cols] = value.astype(BF)
                return carry

            lax.fori_loop(0, n_out, body, 0)

        into(theirs[w], 1 - c)
        landed = passed.at[w, :, low:high]
        send(yes, theirs[w].at[:, low:high], landed, ("p", w, h), partner)
        into(mine[w], c)
        arrive(yes, landed, ("p", w, h), partner)

    def add(when, w, h, at, extra):
        low, high = bounds[h]

        @pl.when(when)
        def _():
            def body(i, carry):
                rows = span(at * block + i * ROWS, ROWS)
                value = mine[w][rows, low:high].astype(F32)
                value = value + passed[w, rows, low:high].astype(F32)
                for n in extra:
                    more = slots[w, n, span(i * ROWS, ROWS), low:high]
                    value = value + more.astype(F32)
                mine[w][rows, low:high] = value.astype(BF)
                return carry

            lax.fori_loop(0, block // ROWS, body, 0)

    def slot(side, step):
        return step - 1 if side == 0 or step == 1 else n_out - 3 + step

    def landing(w, h, side, step):
        low, high = bounds[h]
        return slots.at[w, slot(side, step), :, low:high]

    def summed(w, h, at):
        low, high = bounds[h]
        return mine[w].at[span(at * block, block), low:high]

    ways = (
        (lambda step: jnp.minimum(z + n_out - step, last), ahead, behind),
        (lambda step: jnp.maximum(z - n_out + step, 0), behind, ahead),
    )

    def launch(w, h):
        for step in range(1, n_out):
            for side, when in ((0, z == 0), (1, z == last)):
                at, where, _ = ways[side]
                add(when, w, h, at(step), ())
                there = landing(w, h, side, step)
                send(when, summed(w, h, at(step)), there, ("r", side, w, h, step), where)

    def chain(w, h, step):
        for side, when in ((0, (z > 0) & (z < step)), (1, (z < last) & (z >= n_out - step))):
            at, where, back = ways[side]
            there = landing(w, h, side, step - 1)
            arrive(when, there, ("r", side, w, h, step - 1), back)
            add(when, w, h, at(step), (slot(side, step - 1),))
            there = landing(w, h, side, step)
            send(when, summed(w, h, at(step)), there, ("r", side, w, h, step), where)

    def finish(w, h):
        low, high = bounds[h]
        arrive(z > 0, landing(w, h, 0, last), ("r", 0, w, h, last), behind)
        arrive(z < last, landing(w, h, 1, last), ("r", 1, w, h, last), ahead)
        both = (z > 0) & (z < last)
        add(both, w, h, z, (slot(0, last), slot(1, last)))
        add(z == 0, w, h, z, (slot(1, last),))
        add(z == last, w, h, z, (slot(0, last),))
        rows = summed(w, h, z)
        target = grads.at[w, x, :, low:high]
        local(home, rows, target, ("f", w, h), False)
        send(away, rows, target, ("f", w, h), flipped)
        send(home, rows, target, ("fc", w, h), over_x)
        if (w, h) == final:
            send(away, rows, target, ("fd", w, h), crossed)

    final = (2, 1)

    def pass_on(w, h):
        low, high = bounds[h]
        target = grads.at[w, x, :, low:high]
        arrive(away, target, ("f", w, h), flipped)
        send(away, target, target, ("fd", w, h), over_x)

    def wait_finish(w, h):
        low, high = bounds[h]
        target = grads.at[w, x, :, low:high]
        other = grads.at[w, 1 - x, :, low:high]
        local(home, summed(w, h, z), target, ("f", w, h), True)
        arrive(home, other, ("fc", w, h), over_x)
        if (w, h) == final:
            arrive(away, target, ("f", w, h), flipped)
        arrive(away, other, ("fd", w, h), crossed if (w, h) == final else over_x)

    def make_partial(a):
        def body(i, carry):
            rows = span(a * tokens + (i // (width // tall)) * tall, tall)
            cols = pl.multiple_of((i % (width // tall)) * tall, 128)
            dims = (((1,), (1,)), ((), ()))
            value = lax.dot_general(
                gate[rows, :],
                weights[1, pl.ds(cols, tall), :],
                dims,
                preferred_element_type=F32,
            )
            value = value + lax.dot_general(
                upper[rows, :],
                weights[2, pl.ds(cols, tall), :],
                dims,
                preferred_element_type=F32,
            )
            ys[rows, pl.ds(cols, tall)] = value.astype(BF)
            return carry

        lax.fori_loop(0, (tokens // tall) * (width // tall), body, 0)

    def partial_piece(a, e):
        share = width // n_in
        return ys.at[span(a * tokens, tokens), pl.ds(pl.multiple_of(e * share, 128), share)]

    def send_partial(a, first):
        target = shares.at[x * n_in + y]
        near, far = device(a, z, c, c), device(a, z, c, 1 - c)
        if first == 0:
            local(home, partial_piece(a, c), target, ("i",), False)
        for side in range(n_in):
            here = (y == side) & (away if first == 0 else yes)
            send(here, partial_piece(a, c), target, ("i", first, side), near)
            send(y == side, partial_piece(a, 1 - c), target, ("i", first + 1, side), far)

    def wait_partial():
        local(home, partial_piece(x, c), shares.at[x * n_in + y], ("i",), True)
        for side in range(n_in):
            near = shares.at[x * n_in + side]
            far = shares.at[(1 - x) * n_in + side]
            arrive(home & (y != side), near, ("i", 0, side), device(x, z, side, y))
            arrive(away, near, ("i", 1, side), device(x, z, side, y))
            arrive(home, far, ("i", 2, side), device(1 - x, z, side, y))
            arrive(away, far, ("i", 3, side), device(1 - x, z, side, y))

    def add_partial():
        wide = width // n_in
        places = [(a, d) for a in range(2) for d in range(n_in)]

        def load(a, d):
            there = xs.at[span(a * tokens, tokens), d * wide : (d + 1) * wide]
            k = recv_sems.at[key("load", a, d)]
            return pltpu.make_async_copy(shares.at[a * n_in + d], there, k)

        for place in places:
            load(*place).start()
        for place in places:
            load(*place).wait()

        def body(i, carry):
            value = None
            for a, d in places:
                rows = span(a * tokens + i * ROWS, ROWS)
                more = xs[rows, d * wide : (d + 1) * wide].astype(F32)
                value = more if value is None else value + more
            xs[span(i * ROWS, ROWS), :wide] = value.astype(BF)
            return carry

        lax.fori_loop(0, tokens // ROWS, body, 0)
        out = pltpu.make_async_copy(
            xs.at[span(0, tokens), :wide], grad, recv_sems.at[key("out")]
        )
        out.start()
        out.wait()

    def factor(n):
        return factors[n][0].at[:, pl.ds(pl.multiple_of(x * part, 128), part)]

    send_quarter(0)
    near_over_x(home, 0, cot, ys)
    near_over_y(0, cot, ys)
    keep_near(0, cot, ys)
    for w in range(1, 3):
        narrow(w)
        send_quarter(w)
    for n in range(3):
        local(home, factor(n), factors[n][1], ("s", n), False)
        send(away, factor(n), factors[n][1], ("s", n), flipped)
    send_kept(0, 0, gate_in, gate)
    send_kept(1, 0, up_in, upper)
    send_crossed(home, 0, 0, 0, gate_in, gate)
    send_crossed(home, 0, 1, 0, up_in, upper)
    keep_near(1, inp, xs)

    start_line(0)
    line_step(0, 1)
    forward_low(0, ys)
    forward_high(0, ys)
    send_crossed(away, 1, 0, 0, gate_in, gate)
    send_crossed(away, 1, 1, 0, up_in, upper)
    near_over_x(away, 1, inp, xs)
    near_over_y(1, inp, xs)
    line_step(0, 2)
    start_line(1)
    for step in range(3, n_out):
        line_step(0, step)
    start_line(2)
    line_step(1, 1)

    for n in range(3):
        local(home, factor(n), factors[n][1], ("s", n), True)
        arrive(away, factors[n][1], ("s", n), flipped)
    wait_tokens(0, cot, ys)
    wait_pre(0, 0, gate_in, gate)
    wait_pre(1, 0, up_in, upper)
    make_hidden(0)
    product(0, 0, ys, hidden)
    launch(0, 0)
    line_step(1, 2)
    wait_shared(0)
    drain(lambda name: name[0] == "q" or name[:2] in (("a", 0), ("b", 0), ("d", 0)))
    make_cots(0)
    forward_low(1, xs)
    line_step(2, 1)
    chain(0, 0, 2)
    forward_high(1, xs)
    send_kept(0, 1, gate_in, gate)
    send_kept(1, 1, up_in, upper)
    for step in range(3, n_out):
        line_step(1, step)
    send_crossed(away, 1, 0, 1, gate_in, gate)
    send_crossed(away, 1, 1, 1, up_in, upper)
    for step in range(3, n_out):
        chain(0, 0, step)
    wait_tokens(1, inp, xs)
    product(1, 0, xs, gate)
    send_crossed(home, 0, 0, 1, gate_in, gate)
    send_crossed(home, 0, 1, 1, up_in, upper)
    launch(1, 0)
    product(2, 0, xs, upper)
    launch(2, 0)
    line_step(2, 2)
    finish(0, 0)
    chain(1, 0, 2)

    wait_pre(0, 1, gate_in, gate)
    wait_pre(1, 1, up_in, upper)
    make_hidden(1)
    product(0, 1, ys, hidden)
    launch(0, 1)
    for step in range(3, n_out):
        chain(1, 0, step)
        line_step(2, step)
    make_cots(1)
    wait_shared(1)
    wait_shared(2)
    drain(lambda name: name in (("tl", 0), ("th", 0)))
    pass_on(0, 0)
    make_partial(1 - x)
    send_partial(1 - x, 2)
    chain(2, 0, 2)
    finish(1, 0)
    make_partial(x)
    send_partial(x, 0)
    for step in range(3, n_out):
        chain(2, 0, step)
    product(1, 1, xs, gate)
    launch(1, 1)
    pass_on(1, 0)
    chain(0, 1, 2)
    finish(2, 0)
    product(2, 1, xs, upper)
    launch(2, 1)
    for step in range(3, n_out):
        chain(0, 1, step)
    chain(1, 1, 2)
    finish(0, 1)
    for step in range(3, n_out):
        chain(1, 1, step)
    chain(2, 1, 2)
    finish(1, 1)
    for step in range(3, n_out):
        chain(2, 1, step)
    pass_on(2, 0)
    pass_on(0, 1)
    finish(2, 1)
    pass_on(1, 1)
    wait_partial()
    drain(lambda name: name in (("tl", 1), ("th", 1)))
    add_partial()
    for h in range(2):
        for w in range(3):
            wait_finish(w, h)
    drain(lambda name: True)


def shared(
    n_rep,
    n_fs,
    n_tp,
    inputs,
    cotangent,
    gate_pre,
    up_pre,
    gate_weight,
    up_weight,
    down_weight,
    gate_scale,
    up_scale,
    down_scale,
):
    n_in = n_tp
    n_out = n_fs // n_in
    tokens, width = inputs.shape
    block = width // n_fs
    part = gate_pre.shape[1] // n_rep
    half = width // 2
    x = lax.axis_index("rep")

    n_sems = 192
    grads, _, grad = pl.pallas_call(
        functools.partial(whole_step, n_in, n_out),
        out_shape=(
            jax.ShapeDtypeStruct((3, n_rep, block, part), BF),
            jax.ShapeDtypeStruct((n_rep * n_in, tokens, width // n_tp), BF),
            jax.ShapeDtypeStruct((tokens, width // n_tp), BF),
        ),
        in_specs=[pl.BlockSpec(memory_space=pltpu.HBM)] * 10,
        out_specs=(
            pl.BlockSpec(memory_space=pltpu.HBM),
            pl.BlockSpec(memory_space=pltpu.HBM),
            pl.BlockSpec(memory_space=pltpu.HBM),
        ),
        scratch_shapes=[
            pltpu.VMEM((3, width, part), BF),
            pltpu.VMEM((2 * tokens, part), BF),
            pltpu.VMEM((2 * tokens, part), BF),
            pltpu.VMEM((2 * tokens, width), BF),
            pltpu.VMEM((2 * tokens, width), BF),
            pltpu.VMEM((2 * tokens, part), BF),
            pltpu.VMEM((half, part), BF),
            pltpu.VMEM((half, part), BF),
            pltpu.VMEM((half, part), BF),
            pltpu.VMEM((3, half, part), BF),
            pltpu.VMEM((3, 2 * n_out - 3, block, part), BF),
            pltpu.VMEM((1, part), F32),
            pltpu.VMEM((1, part), F32),
            pltpu.VMEM((1, part), F32),
            pltpu.VMEM((block, part), F32),
            pltpu.SemaphoreType.DMA((n_sems,)),
            pltpu.SemaphoreType.DMA((n_sems,)),
        ],
        compiler_params=pltpu.CompilerParams(
            collective_id=0, has_side_effects=True, vmem_limit_bytes=67043328
        ),
    )(
        cotangent,
        inputs,
        gate_pre,
        up_pre,
        down_weight,
        gate_weight,
        up_weight,
        gate_scale,
        up_scale,
        down_scale,
    )
    wide = [
        jnp.concatenate([grads[w, p] for p in range(n_rep)], axis=1).astype(F32)
        for w in range(3)
    ]
    return (grad, wide[1], wide[2], wide[0])


def fits(sizes, arrays):
    n_rep, n_fs, n_tp = sizes
    tokens, width = arrays[0].shape
    part = arrays[2].shape[1] // n_rep
    return (
        n_rep == 2
        and n_tp == 2
        and n_fs == 8
        and part % 128 == 0
        and width % (n_fs * 128) == 0
        and tokens % 256 == 0
    )


def local_step(sizes, *arrays):
    body = shared if fits(sizes, arrays) else local
    return body(*sizes, *arrays)


def solution(mesh):
    sizes = mesh.shape
    return jax.shard_map(
        functools.partial(local_step, (sizes["rep"], sizes["fs"], sizes["tp"])),
        mesh=mesh,
        in_specs=(
            P(("rep", "fs"), None),
            P(("rep", "fs"), None),
            P(("rep", "fs"), "tp"),
            P(("rep", "fs"), "tp"),
            P("fs", "tp"),
            P("fs", "tp"),
            P("fs", "tp"),
            P(None, "tp"),
            P(None, "tp"),
            P(None, "tp"),
        ),
        out_specs=(P(("rep", "fs"), "tp"), P("fs", "tp"), P("fs", "tp"), P("fs", "tp")),
        check_vma=False,
    )
```

```python
import functools

import jax
import jax.numpy as jnp
from jax import lax
from jax.experimental import pallas as pl
from jax.experimental.pallas import tpu as pltpu
from jax.sharding import PartitionSpec as P


BF = jnp.bfloat16
F32 = jnp.float32


def local(
    n_rep,
    n_fs,
    n_tp,
    inputs,
    cotangent,
    gate_pre,
    up_pre,
    gate_weight,
    up_weight,
    down_weight,
    gate_scale,
    up_scale,
    down_scale,
):
    n_out = 4 if n_fs % 4 == 0 else 1
    n_in = n_fs // n_out
    tokens = inputs.shape[0]
    width = inputs.shape[1]
    block = width // n_fs
    part = gate_pre.shape[1] // n_rep
    r = lax.axis_index("rep")
    f = lax.axis_index("fs")
    t = lax.axis_index("tp")
    zo, yo = f // n_in, f % n_in

    def from_rep(value, k):
        return lax.ppermute(value, "rep", [((i + k) % n_rep, i) for i in range(n_rep)])

    def from_tp(value, k):
        return lax.ppermute(value, "tp", [((i + k) % n_tp, i) for i in range(n_tp)])

    def from_outer(value, k):
        pairs = [
            (((z + k) % n_out) * n_in + y, z * n_in + y)
            for z in range(n_out)
            for y in range(n_in)
        ]
        return lax.ppermute(value, "fs", pairs)

    def from_inner(value, k):
        pairs = [
            (z * n_in + (y + k) % n_in, z * n_in + y)
            for z in range(n_out)
            for y in range(n_in)
        ]
        return lax.ppermute(value, "fs", pairs)

    def column_part(value, index):
        return lax.dynamic_slice_in_dim(value, index * part, part, 1)

    def spread_tokens(value):
        return jnp.concatenate([value] + [from_rep(value, k) for k in range(1, n_rep)], axis=0)

    def exchange_parts(value):
        pieces = [column_part(value, r)]
        for k in range(1, n_rep):
            pieces.append(from_rep(column_part(value, (r - k + n_rep) % n_rep), k))
        return jnp.concatenate(pieces, axis=0)

    def rotate(value):
        result = []
        for j in range(n_in):
            cuts = [
                lax.dynamic_slice_in_dim(
                    value, (((zo + i) % n_out) * n_in + (yo + j) % n_in) * block, block, 1
                )
                for i in range(n_out)
            ]
            result.append(jnp.concatenate(cuts, axis=1))
        return jnp.concatenate(result, axis=1)

    def gather_rows(own):
        line = [own] + [from_outer(own, i) for i in range(1, n_out)]
        blocks = list(line)
        for j in range(1, n_in):
            blocks += [from_inner(b, j) for b in line]
        return jnp.concatenate(blocks, axis=0)

    down_all = gather_rows(column_part(down_weight, r).astype(BF))
    gate = exchange_parts(gate_pre).astype(F32)
    upper = exchange_parts(up_pre).astype(F32)
    ys = spread_tokens(rotate(cotangent))
    xs = spread_tokens(rotate(inputs))
    gs, us, ds = (column_part(s, r) for s in (gate_scale, up_scale, down_scale))

    sig = jax.nn.sigmoid(gate)
    act = gate * sig
    hidden = (act * upper).astype(BF)
    hidden_cot = jnp.dot(ys, down_all, preferred_element_type=F32) * ds
    gate_cot = (hidden_cot * upper * sig * (1.0 + gate * (1.0 - sig)) * gs).astype(BF)
    up_cot = (hidden_cot * act * us).astype(BF)
    both_cot = jnp.concatenate([gate_cot, up_cot], axis=1)

    dims = (((0,), (0,)), ((), ()))
    stretch = n_out * block

    def scattered(left, right, scale):
        def piece(j):
            value = lax.dot_general(
                left[:, j * stretch : (j + 1) * stretch], right, dims, preferred_element_type=F32
            )
            if scale is not None:
                value = value * scale
            return value

        arrived = []
        for j in range(1, n_in):
            arrived.append(from_inner(piece(j).astype(BF), n_in - j))
        total = piece(0)
        for value in arrived:
            total = total + value.astype(F32)
        own = total[:block]
        sent = total[block:].astype(BF)
        for i in range(1, n_out):
            own = own + from_outer(sent[(i - 1) * block : i * block], n_out - i).astype(F32)
        return lax.reduce_precision(own, 8, 7)

    def whole_columns(own):
        result = jnp.zeros((block, part * n_rep), F32)
        narrow = own.astype(BF)
        result = lax.dynamic_update_slice_in_dim(result, own, r * part, 1)
        for k in range(1, n_rep):
            value = from_rep(narrow, k).astype(F32)
            result = lax.dynamic_update_slice_in_dim(result, value, ((r + k) % n_rep) * part, 1)
        return result

    down_grad = whole_columns(scattered(ys, hidden, ds))
    gate_grad = whole_columns(scattered(xs, gate_cot, None))
    up_grad = whole_columns(scattered(xs, up_cot, None))

    both_rows = jnp.concatenate([column_part(gate_weight, r), column_part(up_weight, r)], axis=1)
    both_all = gather_rows(both_rows.astype(BF))
    partial = lax.dot_general(
        both_cot, both_all, (((1,), (1,)), ((), ())), preferred_element_type=F32
    ).astype(BF)
    back = []
    for z in range(n_out):
        for y in range(n_in):
            i = (z - zo + n_out) % n_out
            j = (y - yo + n_in) % n_in
            back.append(lax.dynamic_slice_in_dim(partial, (j * n_out + i) * block, block, 1))
    partial = jnp.concatenate(back, axis=1)
    share = width // n_tp
    total = lax.dynamic_slice_in_dim(partial, t * share, share, 1).astype(F32)
    for k in range(1, n_tp):
        target = (t - k + n_tp) % n_tp
        total = total + from_tp(
            lax.dynamic_slice_in_dim(partial, target * share, share, 1), k
        ).astype(F32)
    grad = total[:tokens]
    away = total[tokens:].astype(BF)
    for k in range(1, n_rep):
        grad = grad + from_rep(away[(k - 1) * tokens : k * tokens], n_rep - k).astype(F32)
    return (grad.astype(BF), gate_grad, up_grad, down_grad)


MESH = pl.DeviceIdType.MESH
ROWS = 32


def span(start, size):
    return pl.ds(pl.multiple_of(start, 16), size)


def whole_step(
    n_in,
    n_out,
    cot,
    inp,
    gate_in,
    up_in,
    down_weight,
    gate_weight,
    up_weight,
    gate_factor,
    up_factor,
    down_factor,
    down_out,
    gate_out,
    up_out,
    shares,
    grad,
    weights,
    gate,
    upper,
    ys,
    xs,
    hidden,
    own_down,
    own_up,
    away_down,
    passed,
    slots,
    gate_scales,
    up_scales,
    down_scales,
    staged,
    send_sems,
    recv_sems,
):
    x = lax.axis_index("rep")
    f = lax.axis_index("fs")
    c = lax.axis_index("tp")
    z, y = f // n_in, f % n_in
    home = c == y
    away = c != y
    tokens, width = cot.shape
    part = gate.shape[1]
    block = width // (n_in * n_out)
    half = width // 2
    last = n_out - 1

    def device(a, b, d, e):
        return (a, b * n_in + d, e)

    keys = {}
    sent = []

    def key(*name):
        return keys.setdefault(name, len(keys))

    def remote(source, target, name, where):
        k = key(*name)
        return pltpu.make_async_remote_copy(
            src_ref=source,
            dst_ref=target,
            send_sem=send_sems.at[k],
            recv_sem=recv_sems.at[k],
            device_id=where,
            device_id_type=MESH,
        )

    def send(when, source, target, name, where):
        @pl.when(when)
        def _():
            remote(source, target, name, where).start()

        sent.append((name, when, source, target, where))

    def arrive(when, target, name, where):
        @pl.when(when)
        def _():
            remote(target, target, name, where).wait_recv()

    def drain(chosen):
        rest = []
        for entry in sent:
            name, when, source, target, where = entry
            if not chosen(name):
                rest.append(entry)
                continue

            @pl.when(when)
            def _():
                remote(source, target, name, where).wait_send()

        sent[:] = rest

    def local(when, source, target, name, wait):
        @pl.when(when)
        def _():
            copy = pltpu.make_async_copy(source, target, recv_sems.at[key("local", *name)])
            if wait:
                copy.wait()
            else:
                copy.start()

    yes = x >= 0
    stored = (down_weight, gate_weight, up_weight)
    factors = (
        (gate_factor, gate_scales),
        (up_factor, up_scales),
        (down_factor, down_scales),
    )
    flipped = device(x, z, c, y)
    crossed = device(1 - x, z, c, y)
    over_x = device(1 - x, z, y, c)
    over_y = device(x, z, 1 - y, c)
    partner = device(x, z, y, 1 - c)
    ahead = device(x, jnp.minimum(z + 1, last), y, c)
    behind = device(x, jnp.maximum(z - 1, 0), y, c)

    def load_stored(w):
        quarter = stored[w].at[:, pl.ds(pl.multiple_of(x * part, 128), part)]
        return pltpu.make_async_copy(quarter, staged, recv_sems.at[key("w", w)])

    def narrowed(w):
        return own_up.at[w * block : (w + 1) * block]

    def narrow(w):
        load_stored(w).wait()

        def into(target, base):
            def body(i, carry):
                rows = staged[span(i * ROWS, ROWS), :].astype(BF)
                target[span(base + i * ROWS, ROWS), :] = rows
                return carry

            lax.fori_loop(0, block // ROWS, body, 0)

        @pl.when(home)
        def _():
            into(weights.at[w], (z * n_in + c) * block)

        @pl.when(away)
        def _():
            into(own_up, w * block)

        if w < 2:
            load_stored(w + 1).start()

    load_stored(0).start()

    barrier = pltpu.get_barrier_semaphore()
    for i in range(1, 8):
        other = device((x + i // 4) % 2, z, (y + (i // 2) % 2) % 2, (c + i % 2) % 2)
        pl.semaphore_signal(barrier, inc=1, device_id=other, device_id_type=MESH)

    @pl.when(z < last)
    def _():
        pl.semaphore_signal(barrier, inc=1, device_id=ahead, device_id_type=MESH)

    @pl.when(z > 0)
    def _():
        pl.semaphore_signal(barrier, inc=1, device_id=behind, device_id_type=MESH)

    narrow(0)
    pl.semaphore_wait(barrier, 7 + (z < last).astype(jnp.int32) + (z > 0).astype(jnp.int32))

    def weight_rows(w, at, side):
        return weights.at[w, span((at * n_in + side) * block, block)]

    def send_quarter(w):
        send(away, narrowed(w), weight_rows(w, z, y), ("q", w), flipped)

    def wait_quarter(w):
        arrive(away, weight_rows(w, z, c), ("q", w), flipped)

    cuts = (tokens // 8, tokens // 8 * 3)

    def piece(index, target, a, high):
        cut = cuts[index]
        if high:
            return target.at[span(a * tokens + cut, tokens - cut)]
        return target.at[span(a * tokens, cut)]

    def keep_near(index, source, target):
        local(home, source, target.at[span(x * tokens, tokens)], ("t", index), False)

    def near_over_x(when, index, source, target):
        where = device(1 - x, z, y, y)
        for high in (0, 1):
            rows = piece(index, target, x, high)
            send(when, piece(index, source, 0, high), rows, ("tx", index, high), where)

    def near_over_y(index, source, target):
        for high in (1, 0):
            rows = piece(index, target, x, high)
            send(away, piece(index, source, 0, high), rows, ("ty", index, high), flipped)

    def forward_low(index, target):
        low = piece(index, target, 1 - x, 0)
        arrive(home, low, ("tx", index, 0), over_x)
        send(home, low, low, ("tl", index), over_y)

    def forward_high(index, target):
        high = piece(index, target, x, 1)
        arrive(away, high, ("ty", index, 1), flipped)
        send(away, high, high, ("th", index), over_x)

    def wait_tokens(index, source, target):
        local(home, source, target.at[span(x * tokens, tokens)], ("t", index), True)
        arrive(home, piece(index, target, 1 - x, 1), ("tx", index, 1), over_x)
        arrive(away, piece(index, target, x, 0), ("ty", index, 0), flipped)
        arrive(away, piece(index, target, 1 - x, 0), ("tl", index), over_y)
        arrive(away, piece(index, target, 1 - x, 1), ("th", index), over_x)

    middle = (part // 128 + 1) // 2 * 128
    bounds = ((0, middle), (middle, part))

    def columns(source, p, h):
        low, high = bounds[h]
        return source.at[:, pl.ds(pl.multiple_of(p * part + low, 128), high - low)]

    def pre_rows(target, a, h):
        low, high = bounds[h]
        return target.at[span(a * tokens, tokens), low:high]

    def send_kept(index, h, source, target):
        rows = pre_rows(target, x, h)
        local(home, columns(source, x, h), rows, ("ga", index, h), False)
        send(away, columns(source, x, h), rows, ("ga", index, h), flipped)

    def send_crossed(when, which, index, h, source, target):
        rows = pre_rows(target, x, h)
        send(when, columns(source, 1 - x, h), rows, ("gb", index, h, which), crossed)

    def wait_pre(index, h, source, target):
        near = pre_rows(target, x, h)
        far = pre_rows(target, 1 - x, h)
        local(home, columns(source, x, h), near, ("ga", index, h), True)
        arrive(away, near, ("ga", index, h), flipped)
        arrive(home, far, ("gb", index, h, 0), over_x)
        arrive(away, far, ("gb", index, h, 1), crossed)

    def share_block(w, step, side, at, when):
        rows = weight_rows(w, at, c)
        send(when, rows, rows, ("d", w, step, side), partner)

    def start_line(w):
        wait_quarter(w)
        rows = weight_rows(w, z, c)
        send(z < last, rows, rows, ("a", w, 1), ahead)
        send(z > 0, rows, rows, ("b", w, 1), behind)
        share_block(w, 0, 0, z, yes)

    def line_step(w, step):
        rows = weight_rows(w, jnp.maximum(z - step, 0), c)
        arrive(z >= step, rows, ("a", w, step), behind)
        if step < last:
            send((z >= step) & (z < last), rows, rows, ("a", w, step + 1), ahead)
        share_block(w, step, 1, jnp.maximum(z - step, 0), z >= step)
        rows = weight_rows(w, jnp.minimum(z + step, last), c)
        arrive(z + step <= last, rows, ("b", w, step), ahead)
        if step < last:
            send((z + step <= last) & (z > 0), rows, rows, ("b", w, step + 1), behind)
        share_block(w, step, 2, jnp.minimum(z + step, last), z + step <= last)

    def wait_shared(w):
        arrive(yes, weight_rows(w, z, 1 - c), ("d", w, 0, 0), partner)
        for step in range(1, n_out):
            arrive(
                z >= step,
                weight_rows(w, jnp.maximum(z - step, 0), 1 - c),
                ("d", w, step, 1),
                partner,
            )
            arrive(
                z + step <= last,
                weight_rows(w, jnp.minimum(z + step, last), 1 - c),
                ("d", w, step, 2),
                partner,
            )

    def tiles(h):
        low, high = bounds[h]
        return [(at, min(256, high - at)) for at in range(low, high, 256)]

    pair = 2 * tokens
    tall = 256

    def make_hidden(h):
        def body(i, carry):
            rows = span(i * 64, 64)
            for at, size in tiles(h):
                g = gate[rows, at : at + size].astype(F32)
                u = upper[rows, at : at + size].astype(F32)
                hidden[rows, at : at + size] = (g * jax.nn.sigmoid(g) * u).astype(BF)
            return carry

        lax.fori_loop(0, pair // 64, body, 0)

    def make_cots(h):
        def body(i, carry):
            rows = span(i * tall, tall)
            for at, size in tiles(h):
                cols = slice(at, at + size)
                value = jnp.dot(ys[rows, :], weights[0, :, cols], preferred_element_type=F32)
                value = value * down_scales[:, cols]
                g = gate[rows, cols].astype(F32)
                u = upper[rows, cols].astype(F32)
                sig = jax.nn.sigmoid(g)
                act = g * sig
                slope = value * u * sig * (1.0 + g * (1.0 - sig)) * gate_scales[:, cols]
                gate[rows, cols] = slope.astype(BF)
                upper[rows, cols] = (value * act * up_scales[:, cols]).astype(BF)
            return carry

        lax.fori_loop(0, pair // tall, body, 0)

    mine = (own_down, hidden, own_up)
    theirs = (away_down, weights.at[0, :half], weights.at[0, half:])

    def product(w, h, left, right):
        low, high = bounds[h]


        def into(target, side):
            def body(i, carry):
                at = pl.multiple_of((i * n_in + side) * block, 128)
                a = left[:, pl.ds(at, block)]
                for start, size in tiles(h):
                    cols = slice(start, start + size)
                    value = lax.dot_general(
                        a, right[:, cols], (((0,), (0,)), ((), ())), preferred_element_type=F32
                    )
                    if w == 0:
                        value = value * down_scales[:, cols]
                    target[span(i * block, block), cols] = value.astype(BF)
                return carry

            lax.fori_loop(0, n_out, body, 0)

        into(theirs[w], 1 - c)
        landed = passed.at[w, :, low:high]
        send(yes, theirs[w].at[:, low:high], landed, ("p", w, h), partner)
        into(mine[w], c)
        arrive(yes, landed, ("p", w, h), partner)

    def add(when, w, h, at, extra):
        low, high = bounds[h]

        @pl.when(when)
        def _():
            def body(i, carry):
                rows = span(at * block + i * ROWS, ROWS)
                value = mine[w][rows, low:high].astype(F32)
                value = value + passed[w, rows, low:high].astype(F32)
                for n in extra:
                    more = slots[w, n, span(i * ROWS, ROWS), low:high]
                    value = value + more.astype(F32)
                mine[w][rows, low:high] = value.astype(BF)
                return carry

            lax.fori_loop(0, block // ROWS, body, 0)

    def slot(side, step):
        return step - 1 if side == 0 or step == 1 else n_out - 3 + step

    def landing(w, h, side, step):
        low, high = bounds[h]
        return slots.at[w, slot(side, step), :, low:high]

    def summed(w, h, at):
        low, high = bounds[h]
        return mine[w].at[span(at * block, block), low:high]

    ways = (
        (lambda step: jnp.minimum(z + n_out - step, last), ahead, behind),
        (lambda step: jnp.maximum(z - n_out + step, 0), behind, ahead),
    )

    def launch(w, h):
        for step in range(1, n_out):
            for side, when in ((0, z == 0), (1, z == last)):
                at, where, _ = ways[side]
                add(when, w, h, at(step), ())
                there = landing(w, h, side, step)
                send(when, summed(w, h, at(step)), there, ("r", side, w, h, step), where)

    def chain(w, h, step):
        for side, when in ((0, (z > 0) & (z < step)), (1, (z < last) & (z >= n_out - step))):
            at, where, back = ways[side]
            there = landing(w, h, side, step - 1)
            arrive(when, there, ("r", side, w, h, step - 1), back)
            add(when, w, h, at(step), (slot(side, step - 1),))
            there = landing(w, h, side, step)
            send(when, summed(w, h, at(step)), there, ("r", side, w, h, step), where)

    def out_columns(w, p, h):
        low, high = bounds[h]
        at = pl.multiple_of(p * part + low, 128)
        return (down_out, gate_out, up_out)[w].at[:, pl.ds(at, high - low)]

    def finish(w, h):
        arrive(z > 0, landing(w, h, 0, last), ("r", 0, w, h, last), behind)
        arrive(z < last, landing(w, h, 1, last), ("r", 1, w, h, last), ahead)
        both = (z > 0) & (z < last)
        add(both, w, h, z, (slot(0, last), slot(1, last)))
        add(z == 0, w, h, z, (slot(1, last),))
        add(z == last, w, h, z, (slot(0, last),))
        rows = summed(w, h, z)
        target = out_columns(w, x, h)
        local(home, rows, target, ("f", w, h), False)
        send(away, rows, target, ("f", w, h), flipped)
        send(home, rows, target, ("fc", w, h), over_x)
        if (w, h) == final:
            send(away, rows, target, ("fd", w, h), crossed)

    final = (2, 1)

    def pass_on(w, h):
        target = out_columns(w, x, h)
        arrive(away, target, ("f", w, h), flipped)
        send(away, target, target, ("fd", w, h), over_x)

    def wait_finish(w, h):
        target = out_columns(w, x, h)
        other = out_columns(w, 1 - x, h)
        local(home, summed(w, h, z), target, ("f", w, h), True)
        arrive(home, other, ("fc", w, h), over_x)
        if (w, h) == final:
            arrive(away, target, ("f", w, h), flipped)
        arrive(away, other, ("fd", w, h), crossed if (w, h) == final else over_x)

    def make_partial(a):
        def body(i, carry):
            rows = span(a * tokens + (i // (width // tall)) * tall, tall)
            cols = pl.multiple_of((i % (width // tall)) * tall, 128)
            dims = (((1,), (1,)), ((), ()))
            value = lax.dot_general(
                gate[rows, :],
                weights[1, pl.ds(cols, tall), :],
                dims,
                preferred_element_type=F32,
            )
            value = value + lax.dot_general(
                upper[rows, :],
                weights[2, pl.ds(cols, tall), :],
                dims,
                preferred_element_type=F32,
            )
            ys[rows, pl.ds(cols, tall)] = value.astype(BF)
            return carry

        lax.fori_loop(0, (tokens // tall) * (width // tall), body, 0)

    def partial_piece(a, e):
        share = width // n_in
        return ys.at[span(a * tokens, tokens), pl.ds(pl.multiple_of(e * share, 128), share)]

    def send_partial(a, first):
        target = shares.at[x * n_in + y]
        near, far = device(a, z, c, c), device(a, z, c, 1 - c)
        if first == 0:
            local(home, partial_piece(a, c), target, ("i",), False)
        for side in range(n_in):
            here = (y == side) & (away if first == 0 else yes)
            send(here, partial_piece(a, c), target, ("i", first, side), near)
            send(y == side, partial_piece(a, 1 - c), target, ("i", first + 1, side), far)

    def wait_partial():
        local(home, partial_piece(x, c), shares.at[x * n_in + y], ("i",), True)
        for side in range(n_in):
            near = shares.at[x * n_in + side]
            far = shares.at[(1 - x) * n_in + side]
            arrive(home & (y != side), near, ("i", 0, side), device(x, z, side, y))
            arrive(away, near, ("i", 1, side), device(x, z, side, y))
            arrive(home, far, ("i", 2, side), device(1 - x, z, side, y))
            arrive(away, far, ("i", 3, side), device(1 - x, z, side, y))

    def add_partial():
        wide = width // n_in
        places = [(a, d) for a in range(2) for d in range(n_in)]

        def load(a, d):
            there = xs.at[span(a * tokens, tokens), d * wide : (d + 1) * wide]
            k = recv_sems.at[key("load", a, d)]
            return pltpu.make_async_copy(shares.at[a * n_in + d], there, k)

        for place in places:
            load(*place).start()
        for place in places:
            load(*place).wait()

        def body(i, carry):
            value = None
            for a, d in places:
                rows = span(a * tokens + i * ROWS, ROWS)
                more = xs[rows, d * wide : (d + 1) * wide].astype(F32)
                value = more if value is None else value + more
            xs[span(i * ROWS, ROWS), :wide] = value.astype(BF)
            return carry

        lax.fori_loop(0, tokens // ROWS, body, 0)
        out = pltpu.make_async_copy(
            xs.at[span(0, tokens), :wide], grad, recv_sems.at[key("out")]
        )
        out.start()
        out.wait()

    def factor(n):
        return factors[n][0].at[:, pl.ds(pl.multiple_of(x * part, 128), part)]

    send_quarter(0)
    near_over_x(home, 0, cot, ys)
    near_over_y(0, cot, ys)
    keep_near(0, cot, ys)
    for w in range(1, 3):
        narrow(w)
        send_quarter(w)
    for n in range(3):
        local(home, factor(n), factors[n][1], ("s", n), False)
        send(away, factor(n), factors[n][1], ("s", n), flipped)
    send_kept(0, 0, gate_in, gate)
    send_kept(1, 0, up_in, upper)
    send_crossed(home, 0, 0, 0, gate_in, gate)
    send_crossed(home, 0, 1, 0, up_in, upper)
    keep_near(1, inp, xs)

    start_line(0)
    line_step(0, 1)
    forward_low(0, ys)
    forward_high(0, ys)
    send_crossed(away, 1, 0, 0, gate_in, gate)
    send_crossed(away, 1, 1, 0, up_in, upper)
    near_over_x(away, 1, inp, xs)
    near_over_y(1, inp, xs)
    line_step(0, 2)
    start_line(1)
    for step in range(3, n_out):
        line_step(0, step)
    start_line(2)
    line_step(1, 1)

    for n in range(3):
        local(home, factor(n), factors[n][1], ("s", n), True)
        arrive(away, factors[n][1], ("s", n), flipped)
    wait_tokens(0, cot, ys)
    wait_pre(0, 0, gate_in, gate)
    wait_pre(1, 0, up_in, upper)
    make_hidden(0)
    product(0, 0, ys, hidden)
    launch(0, 0)
    line_step(1, 2)
    wait_shared(0)
    drain(lambda name: name[0] == "q" or name[:2] in (("a", 0), ("b", 0), ("d", 0)))
    make_cots(0)
    forward_low(1, xs)
    line_step(2, 1)
    chain(0, 0, 2)
    forward_high(1, xs)
    send_kept(0, 1, gate_in, gate)
    send_kept(1, 1, up_in, upper)
    for step in range(3, n_out):
        line_step(1, step)
    send_crossed(away, 1, 0, 1, gate_in, gate)
    send_crossed(away, 1, 1, 1, up_in, upper)
    for step in range(3, n_out):
        chain(0, 0, step)
    wait_tokens(1, inp, xs)
    product(1, 0, xs, gate)
    send_crossed(home, 0, 0, 1, gate_in, gate)
    send_crossed(home, 0, 1, 1, up_in, upper)
    launch(1, 0)
    product(2, 0, xs, upper)
    launch(2, 0)
    line_step(2, 2)
    finish(0, 0)
    chain(1, 0, 2)

    wait_pre(0, 1, gate_in, gate)
    wait_pre(1, 1, up_in, upper)
    make_hidden(1)
    product(0, 1, ys, hidden)
    launch(0, 1)
    for step in range(3, n_out):
        chain(1, 0, step)
        line_step(2, step)
    make_cots(1)
    wait_shared(1)
    wait_shared(2)
    drain(lambda name: name in (("tl", 0), ("th", 0)))
    pass_on(0, 0)
    make_partial(1 - x)
    send_partial(1 - x, 2)
    chain(2, 0, 2)
    finish(1, 0)
    make_partial(x)
    send_partial(x, 0)
    for step in range(3, n_out):
        chain(2, 0, step)
    product(1, 1, xs, gate)
    launch(1, 1)
    pass_on(1, 0)
    chain(0, 1, 2)
    finish(2, 0)
    product(2, 1, xs, upper)
    launch(2, 1)
    for step in range(3, n_out):
        chain(0, 1, step)
    chain(1, 1, 2)
    finish(0, 1)
    for step in range(3, n_out):
        chain(1, 1, step)
    chain(2, 1, 2)
    finish(1, 1)
    for step in range(3, n_out):
        chain(2, 1, step)
    pass_on(2, 0)
    pass_on(0, 1)
    finish(2, 1)
    pass_on(1, 1)
    wait_partial()
    drain(lambda name: name in (("tl", 1), ("th", 1)))
    add_partial()
    for h in range(2):
        for w in range(3):
            wait_finish(w, h)
    drain(lambda name: True)


def shared(
    n_rep,
    n_fs,
    n_tp,
    inputs,
    cotangent,
    gate_pre,
    up_pre,
    gate_weight,
    up_weight,
    down_weight,
    gate_scale,
    up_scale,
    down_scale,
):
    n_in = n_tp
    n_out = n_fs // n_in
    tokens, width = inputs.shape
    block = width // n_fs
    part = gate_pre.shape[1] // n_rep
    half = width // 2
    x = lax.axis_index("rep")

    n_sems = 192
    down_grad, gate_grad, up_grad, _, grad = pl.pallas_call(
        functools.partial(whole_step, n_in, n_out),
        out_shape=(
            jax.ShapeDtypeStruct((block, n_rep * part), BF),
            jax.ShapeDtypeStruct((block, n_rep * part), BF),
            jax.ShapeDtypeStruct((block, n_rep * part), BF),
            jax.ShapeDtypeStruct((n_rep * n_in, tokens, width // n_tp), BF),
            jax.ShapeDtypeStruct((tokens, width // n_tp), BF),
        ),
        in_specs=[pl.BlockSpec(memory_space=pltpu.HBM)] * 10,
        out_specs=(
            pl.BlockSpec(memory_space=pltpu.HBM),
            pl.BlockSpec(memory_space=pltpu.HBM),
            pl.BlockSpec(memory_space=pltpu.HBM),
            pl.BlockSpec(memory_space=pltpu.HBM),
            pl.BlockSpec(memory_space=pltpu.HBM),
        ),
        scratch_shapes=[
            pltpu.VMEM((3, width, part), BF),
            pltpu.VMEM((2 * tokens, part), BF),
            pltpu.VMEM((2 * tokens, part), BF),
            pltpu.VMEM((2 * tokens, width), BF),
            pltpu.VMEM((2 * tokens, width), BF),
            pltpu.VMEM((2 * tokens, part), BF),
            pltpu.VMEM((half, part), BF),
            pltpu.VMEM((half, part), BF),
            pltpu.VMEM((half, part), BF),
            pltpu.VMEM((3, half, part), BF),
            pltpu.VMEM((3, 2 * n_out - 3, block, part), BF),
            pltpu.VMEM((1, part), F32),
            pltpu.VMEM((1, part), F32),
            pltpu.VMEM((1, part), F32),
            pltpu.VMEM((block, part), F32),
            pltpu.SemaphoreType.DMA((n_sems,)),
            pltpu.SemaphoreType.DMA((n_sems,)),
        ],
        compiler_params=pltpu.CompilerParams(
            collective_id=0, has_side_effects=True, vmem_limit_bytes=67043328
        ),
    )(
        cotangent,
        inputs,
        gate_pre,
        up_pre,
        down_weight,
        gate_weight,
        up_weight,
        gate_scale,
        up_scale,
        down_scale,
    )
    return (grad, gate_grad.astype(F32), up_grad.astype(F32), down_grad.astype(F32))


def fits(sizes, arrays):
    n_rep, n_fs, n_tp = sizes
    tokens, width = arrays[0].shape
    part = arrays[2].shape[1] // n_rep
    return (
        n_rep == 2
        and n_tp == 2
        and n_fs == 8
        and part % 128 == 0
        and width % (n_fs * 128) == 0
        and tokens % 256 == 0
    )


def local_step(sizes, *arrays):
    body = shared if fits(sizes, arrays) else local
    return body(*sizes, *arrays)


def solution(mesh):
    sizes = mesh.shape
    return jax.shard_map(
        functools.partial(local_step, (sizes["rep"], sizes["fs"], sizes["tp"])),
        mesh=mesh,
        in_specs=(
            P(("rep", "fs"), None),
            P(("rep", "fs"), None),
            P(("rep", "fs"), "tp"),
            P(("rep", "fs"), "tp"),
            P("fs", "tp"),
            P("fs", "tp"),
            P("fs", "tp"),
            P(None, "tp"),
            P(None, "tp"),
            P(None, "tp"),
        ),
        out_specs=(P(("rep", "fs"), "tp"), P("fs", "tp"), P("fs", "tp"), P("fs", "tp")),
        check_vma=False,
    )
```
